32 devices in a mesh: sp: 8 (over z, y), tp: 4 (over x, core).
Axes of the slice: x: 2, y: 2, z: 4, core: 2. Of those that a mesh axis runs over, the one named last changes fastest.
Arguments:
- latent: bfloat16 [2048, 2048], P('sp'), may hold values from -6 to 6
- context: bfloat16 [1024, 2048], P('sp'), may hold values from -6 to 6
- condition: bfloat16 [2048], replicated, may hold values from -6 to 6
- context_condition: bfloat16 [2048], replicated, may hold values from -6 to 6
- gain_pre: float32 [2048], replicated, may hold values from 0.1 to 1.9
- gain_post: float32 [2048], replicated, may hold values from 0.1 to 1.9
- w_shift: bfloat16 [2048, 2048], P('sp', 'tp'), may hold values from -0.125 to 0.125
- w_scale: bfloat16 [2048, 2048], P('sp', 'tp'), may hold values from -0.125 to 0.125
- w_gate: bfloat16 [2048, 2048], P('sp', 'tp'), may hold values from -0.125 to 0.125
- w_query: bfloat16 [2048, 2048], P(None, 'tp'), may hold values from -0.13258252 to 0.13258252
- w_key: bfloat16 [2048, 2048], P(None, 'tp'), may hold values from -6.629126 to 6.629126
- w_value: bfloat16 [2048, 2048], P(None, 'tp'), may hold values from -0.125 to 0.125
- w_silu: bfloat16 [2048, 2048], P(None, 'tp'), may hold values from -0.125 to 0.125
- offset_bias: float32 [32, 15, 31], P('tp'), may hold values from 1.5 to 3.5
- w_out: bfloat16 [2048, 2048], P('tp'), may hold values from -0.125 to 0.125
Outputs:
- updated: bfloat16 [2048, 2048], P(('sp', 'tp'))
The draws below stay inside these ranges and needn't reach their ends.
All inputs are finite; a program needn't handle non-finite values.
Results may differ from the reference program's by a relative error of at most 0.01.
Values may be sent and summed in bfloat16 or wider, within the bound.
A program may use at most 64 MiB of HBM per device.

```python
import jax
import jax.numpy as jnp
from jax import lax

D = 2048
HEADS = 32
HEAD_DIM = 64
GRID_W = 64
WIN_ROWS = 8
WIN_COLS = 16
CTX = 1024
TOKENS = 2048
N_TP = 4


def query_key_pair(key):
    base = jax.random.fold_in(key, 7)
    first, second, third = jax.random.split(base, 3)
    spread = D ** (-0.5)
    weight_query = jnp.clip(jax.random.normal(first, (D, D), jnp.float32), -6.0, 6.0) * spread
    weight_key = jnp.clip(jax.random.normal(second, (D, D), jnp.float32), -6.0, 6.0) * spread
    return (weight_query, weight_key)


def draw_w_query(key, part):
    return query_key_pair(key)[0].astype(jnp.bfloat16)


def draw_w_key(key, part):
    return query_key_pair(key)[1].astype(jnp.bfloat16)


def steps_of(key, dims, pieces, smallest, high):
    def one(dim, shards_of):
        steps = jax.random.uniform(jax.random.fold_in(jax.random.fold_in(key, 6), dim), (shards_of,), jnp.float32, smallest / len(pieces), high / len(pieces))
        return jnp.repeat(jnp.exp(steps), dims[dim] // shards_of).reshape((-1,) + (1,) * (len(dims) - dim - 1))

    factor_of = one(*pieces[0])
    for cut in pieces[1:]:
        factor_of = factor_of * one(*cut)
    return factor_of


def scatter_about(stream_key, dims, scale, reach, cuts=(), kind=jnp.bfloat16):
    factor_of = steps_of(stream_key, dims, cuts, -0.22, 0.18) if cuts else 1.0
    values = jax.random.normal(stream_key, dims, jnp.float32) * scale * factor_of
    return jnp.minimum(jnp.maximum(values, -reach), reach).astype(kind)


def setup_inputs(seed: int = 0) -> dict:
    streams_of = jax.random.split(jax.random.key(seed), 16)
    latent = scatter_about(streams_of[0], (TOKENS, D), 1.0, 6.0, ((0, 8),))
    context = scatter_about(streams_of[1], (CTX, D), 1.0, 6.0, ((0, 8),))
    condition = scatter_about(streams_of[2], (D,), 1.0, 6.0)
    context_condition = scatter_about(streams_of[3], (D,), 1.0, 6.0)
    gain_pre = jnp.clip(1.0 + 0.18 * jax.random.normal(streams_of[4], (D,), jnp.float32), 0.1, 1.9)
    gain_post = jnp.clip(1.0 + 0.18 * jax.random.normal(streams_of[5], (D,), jnp.float32), 0.1, 1.9)
    w_shift = scatter_about(streams_of[6], (D, D), D ** -0.5, 0.125, ((0, 8), (1, 4)))
    w_scale = scatter_about(streams_of[7], (D, D), D ** -0.5, 0.125, ((0, 8), (1, 4)))
    w_gate = scatter_about(streams_of[8], (D, D), D ** -0.5, 0.125, ((0, 8), (1, 4)))
    w_query = draw_w_query(jax.random.fold_in(streams_of[15], 71), 0)
    w_key = draw_w_key(jax.random.fold_in(streams_of[15], 71), 0)
    w_value = scatter_about(streams_of[11], (D, D), D ** -0.5, 0.125, ((1, 4),))
    w_silu = scatter_about(streams_of[12], (D, D), D ** -0.5, 0.125, ((1, 4),))
    offset_bias = jnp.clip(1.5 + 2.0 * jax.random.uniform(streams_of[13], (HEADS, 2 * WIN_ROWS - 1, 2 * WIN_COLS - 1), jnp.float32) ** steps_of(streams_of[13], (HEADS, 2 * WIN_ROWS - 1, 2 * WIN_COLS - 1), ((0, 4),), -0.2, 0.2), 1.5, 3.5)
    w_out = scatter_about(streams_of[14], (D, D), D ** -0.5, 0.125, ((0, 4),))
    return {"latent": latent, "context": context, "condition": condition, "context_condition": context_condition, "gain_pre": gain_pre, "gain_post": gain_post, "w_shift": w_shift, "w_scale": w_scale, "w_gate": w_gate, "w_query": w_query, "w_key": w_key, "w_value": w_value, "w_silu": w_silu, "offset_bias": offset_bias, "w_out": w_out}


EPSILON = 1e-06

def rounded(values):
    return lax.optimization_barrier(values.astype(jnp.bfloat16))

def normalize(row_block, gain_row):
    values = row_block.astype(jnp.float32)
    return values * lax.rsqrt(lax.optimization_barrier(jnp.mean(values * values, axis=-1, keepdims=True)) + EPSILON) * gain_row

def project(row_block, weight):
    return rounded(jnp.dot(row_block, weight, preferred_element_type=jnp.float32))

def reference(latent, context, condition, context_condition, gain_pre, gain_post, w_shift, w_scale, w_gate, w_query, w_key, w_value, w_silu, offset_bias, w_out):
    active = jax.nn.silu(jnp.stack([condition, context_condition]).astype(jnp.float32)).astype(jnp.bfloat16)
    shifts = jnp.dot(active, w_shift, preferred_element_type=jnp.float32)
    scales = jnp.dot(active, w_scale, preferred_element_type=jnp.float32)
    gating = jnp.dot(active, w_gate, preferred_element_type=jnp.float32)
    hidden = rounded(normalize(latent, gain_pre) * (1.0 + scales[0]) + shifts[0])
    context_hidden = rounded(normalize(context, gain_pre) * (1.0 + scales[1]) + shifts[1])
    queries = project(hidden, w_query)
    keys_latent = project(hidden, w_key)
    values_latent = project(hidden, w_value)
    silu_gate = project(hidden, w_silu)
    context_keys = project(context_hidden, w_key).reshape(-1, HEADS, HEAD_DIM).astype(jnp.float32)
    context_values = project(context_hidden, w_value).reshape(-1, HEADS, HEAD_DIM).astype(jnp.float32)
    tokens, model_width = latent.shape
    grid_rows = tokens // GRID_W
    score_scale = HEAD_DIM ** (-0.5)
    query_grid = queries.reshape(grid_rows, GRID_W, HEADS, HEAD_DIM)
    key_grid = keys_latent.reshape(grid_rows, GRID_W, HEADS, HEAD_DIM)
    value_grid = values_latent.reshape(grid_rows, GRID_W, HEADS, HEAD_DIM)
    columns = jnp.arange(GRID_W, dtype=jnp.int32)
    col_start = jnp.clip(columns - WIN_COLS // 2, 0, GRID_W - WIN_COLS)
    col_inside = (columns[None, :] >= col_start[:, None]) & (columns[None, :] < col_start[:, None] + WIN_COLS)
    col_offset = jnp.clip(columns[None, :] - columns[:, None] + WIN_COLS - 1, 0, 2 * WIN_COLS - 2)

    def row_step(row_index):
        row_first = jnp.clip(row_index - WIN_ROWS // 2, 0, grid_rows - WIN_ROWS)
        query_row = lax.dynamic_index_in_dim(query_grid, row_index, 0, keepdims=False).astype(jnp.float32)
        key_band = lax.dynamic_slice_in_dim(key_grid, row_first, WIN_ROWS, 0).astype(jnp.float32)
        value_band = lax.dynamic_slice_in_dim(value_grid, row_first, WIN_ROWS, 0).astype(jnp.float32)
        row_offset = row_first + jnp.arange(WIN_ROWS, dtype=jnp.int32) - row_index + WIN_ROWS - 1
        offset_terms = offset_bias[:, row_offset[:, None, None], col_offset[None, :, :]]
        window_scores = jnp.einsum('qhd,vkhd->hqvk', query_row, key_band) * score_scale + jnp.transpose(offset_terms, (0, 2, 1, 3))
        window_scores = jnp.where(col_inside[None, :, None, :], window_scores, -jnp.inf)
        context_scores = jnp.einsum('qhd,jhd->hqj', query_row, context_keys) * score_scale
        maximum = jnp.maximum(lax.optimization_barrier(jnp.max(window_scores, axis=(2, 3))), lax.optimization_barrier(jnp.max(context_scores, axis=2)))
        window_exp = jnp.exp(window_scores - maximum[:, :, None, None])
        context_exp = jnp.exp(context_scores - maximum[:, :, None])
        denominator = lax.optimization_barrier(jnp.sum(window_exp, axis=(2, 3))) + lax.optimization_barrier(jnp.sum(context_exp, axis=2))
        window_weights = rounded(window_exp / denominator[:, :, None, None]).astype(jnp.float32)
        context_weights = rounded(context_exp / denominator[:, :, None]).astype(jnp.float32)
        return jnp.einsum('hqvk,vkhd->qhd', window_weights, value_band) + jnp.einsum('hqj,jhd->qhd', context_weights, context_values)
    attended = lax.map(row_step, jnp.arange(grid_rows, dtype=jnp.int32)).reshape(tokens, model_width)
    gated_heads = rounded(jax.nn.silu(silu_gate.astype(jnp.float32)) * attended)
    group_width = model_width // N_TP
    branch_sum = jnp.zeros((tokens, model_width), jnp.float32)
    for group_index in range(N_TP):
        first_col = group_index * group_width
        term = jnp.dot(gated_heads[:, first_col:first_col + group_width], w_out[first_col:first_col + group_width], preferred_element_type=jnp.float32)
        branch_sum = branch_sum + rounded(term).astype(jnp.float32)
    branch = rounded(branch_sum)
    updated = latent.astype(jnp.float32) + gating[0] * normalize(branch, gain_post)
    return updated.astype(jnp.bfloat16)
```

```python
import functools

import jax
import jax.numpy as jnp
from jax import lax
from jax.experimental import pallas as pl
from jax.experimental.pallas import tpu as pltpu
from jax.sharding import PartitionSpec as P

GRID_W = 64
WIN_ROWS = 8
WIN_COLS = 16
EPSILON = 1e-06
MASKED = -1e30
F32 = jnp.float32
BF16 = jnp.bfloat16
TILE = 512
GROUPS = 4


def remote(src, dst, send, recv, where):
    return pltpu.make_async_remote_copy(
        src_ref=src,
        dst_ref=dst,
        send_sem=send,
        recv_sem=recv,
        device_id=where,
        device_id_type=pl.DeviceIdType.MESH,
    )


def dot(a, b):
    return jnp.dot(a, b, preferred_element_type=F32)


def dot_t(a, b):
    return lax.dot_general(a, b, (((1,), (1,)), ((), ())), preferred_element_type=F32)


def kernel(
    S,
    T,
    cond_hbm,
    ctx_cond_hbm,
    gain_pre_hbm,
    gain_post_hbm,
    bias_hbm,
    latent_hbm,
    context_hbm,
    wsh_hbm,
    wsc_hbm,
    wga_hbm,
    wq_hbm,
    wk_hbm,
    wv_hbm,
    ws_hbm,
    wo_hbm,
    out,
    cond_raw,
    ctx_cond_raw,
    active,
    gain_pre,
    gain_post,
    bias,
    lines,
    lat,
    ctx,
    wmod,
    wall,
    wo,
    part,
    modbuf,
    modfull,
    modrow,
    hid,
    kv_out,
    q_out,
    c_out,
    kv,
    queries,
    ckv,
    gate,
    table,
    att_out,
    att,
    prod,
    mate,
    own_sum,
    cross,
    terms,
    load_sem,
    a_send,
    a_recv,
    b_send,
    b_recv,
    f_send,
    f_recv,
    d_send,
    d_recv,
    kv_send,
    kv_recv,
    q_send,
    q_recv,
    c_send,
    c_recv,
    h_send,
    h_recv,
    o_send,
    o_recv,
    m_send,
    m_recv,
    r_send,
    r_recv,
):
    s = lax.axis_index("sp")
    t = lax.axis_index("tp")
    tokens, width = lat.shape
    n_ctx = hid.shape[0] - tokens
    cols = wo.shape[0]
    in_rows = wmod.shape[1]
    rows = tokens // GRID_W
    G = kv_out.shape[0]
    far = S // G
    X = T // 2
    xi = t // 2
    core = t % 2
    g = s // G
    me = s % G
    partner = {"tp": t + 1 - 2 * core}
    half_width = width // 2
    pairs = table.shape[1]

    def member(d):
        return lax.rem(me + d, G)

    def other(f):
        return lax.rem(g + f, far)

    loads = []

    def load(src, dst):
        copy = pltpu.make_async_copy(src, dst, load_sem.at[len(loads)])
        copy.start()
        loads.append(copy)

    load(cond_hbm, cond_raw)
    load(ctx_cond_hbm, ctx_cond_raw)
    load(wsh_hbm, wmod.at[0])
    load(wsc_hbm, wmod.at[1])
    load(wga_hbm, wmod.at[2])
    load(context_hbm, ctx.at[0])
    load(latent_hbm, lat)
    load(bias_hbm, bias)
    load(gain_pre_hbm, gain_pre)
    load(gain_post_hbm, gain_post)
    for j in range(G):
        load(wk_hbm.at[:, pl.ds(j * 128, 128)], wall.at[:, pl.ds(j * 256, 128)])
        load(wv_hbm.at[:, pl.ds(j * 128, 128)], wall.at[:, pl.ds(j * 256 + 128, 128)])
    load(wq_hbm, wall.at[:, pl.ds(2 * cols, cols)])
    load(ws_hbm, wall.at[:, pl.ds(3 * cols, cols)])
    load(wo_hbm, wo)

    barrier = pltpu.get_barrier_semaphore()
    for d in range(1, S):
        pl.semaphore_signal(
            barrier, inc=1, device_id={"sp": lax.rem(s + d, S)}, device_id_type=pl.DeviceIdType.MESH
        )
    for d in range(1, T):
        pl.semaphore_signal(
            barrier, inc=1, device_id={"tp": lax.rem(t + d, T)}, device_id_type=pl.DeviceIdType.MESH
        )

    pending = []

    def send(copy, cond=None):
        pending.append((cond, copy))
        if cond is None:
            copy.start()
        else:

            @pl.when(cond)
            def _():
                copy.start()

    part[...] = jnp.zeros_like(part)
    loads[0].wait()
    loads[1].wait()
    which = lax.broadcasted_iota(jnp.int32, (16, width), 0)
    active[...] = jnp.where(
        which == 0,
        cond_raw[...].astype(F32).reshape(1, width),
        jnp.where(which == 1, ctx_cond_raw[...].astype(F32).reshape(1, width), 0.0),
    )
    if in_rows % 128 == 0:
        own_cond = active[:, pl.ds(pl.multiple_of(s * in_rows, in_rows), in_rows)]
    else:
        shift = lax.rem(width - s * in_rows, width)
        own_cond = pltpu.roll(active[...], shift, 1)[:, 0:in_rows]
    own_active = (own_cond / (1.0 + jnp.exp(-own_cond))).astype(BF16)
    for i in range(3):
        loads[2 + i].wait()
        part[2 * i : 2 * i + 2, :] = dot(own_active, wmod[i])[0:2]
    loads[5].wait()
    pl.semaphore_wait(barrier, S - 1 + T - 1)

    a_copies = []
    for d in range(1, S):
        copy = remote(
            part, modbuf.at[s], a_send.at[d - 1], a_recv.at[d - 1], {"sp": lax.rem(s + d, S)}
        )
        copy.start()
        a_copies.append(copy)

    def half_of(f, c):
        return ctx.at[f, :, pl.ds(pl.multiple_of(c * half_width, half_width), half_width)]

    for f in range(1, far):
        send(
            remote(
                half_of(0, core),
                half_of(far - f, core),
                f_send.at[far - f - 1],
                f_recv.at[far - f - 1],
                {"sp": other(f) * G + me},
            )
        )

    lane = lax.broadcasted_iota(jnp.int32, (GRID_W, 2 * GRID_W), 1) % GRID_W
    row = lax.broadcasted_iota(jnp.int32, (GRID_W, 2 * GRID_W), 0)
    first = jnp.clip(row - WIN_COLS // 2, 0, GRID_W - WIN_COLS)
    inside = (lane >= first) & (lane < first + WIN_COLS)
    loads[7].wait()
    blank = jnp.zeros((bias.shape[1], GRID_W - bias.shape[2]), F32)
    for p in range(pairs):
        lines[p] = jnp.concatenate([bias[p], blank, bias[p + 1], blank], axis=1)
    for e in range(2):
        for p in range(pairs):
            line = jnp.broadcast_to(lines[p, pl.ds(2 * me + e, 1), :], (GRID_W, 2 * GRID_W))
            rolled = pltpu.roll(line, 2 * GRID_W - (WIN_COLS - 1), 1, stride=1, stride_axis=0)
            table[e, p] = jnp.where(inside, rolled, MASKED)

    modbuf[s] = part[...]
    for copy in a_copies:
        copy.wait()
    modfull[t] = jnp.sum(modbuf[...], axis=0)
    b_copies = []
    for d in range(1, T):
        copy = remote(
            modfull.at[t],
            modfull.at[t],
            b_send.at[d - 1],
            b_recv.at[d - 1],
            {"tp": lax.rem(t + d, T)},
        )
        copy.start()
        b_copies.append(copy)
    for i in range(6, len(loads)):
        if i != 7:
            loads[i].wait()
    for copy in b_copies:
        copy.wait()
    for j in range(T):
        at = slice(j * cols, (j + 1) * cols)
        modrow[:, at] = modfull[j]
        modrow[2:4, at] = gain_pre[:, at] * (1.0 + modfull[j, 2:4])

    def hidden(src, dst, count, kind):
        step = 32

        @pl.loop(0, count // step, unroll=min(4, count // step))
        def _(i):
            at = pl.ds(pl.multiple_of(i * step, step), step)
            v = src[at, :].astype(F32)
            inv = lax.rsqrt(jnp.mean(v * v, axis=-1, keepdims=True) + EPSILON)
            v = v * inv * modrow[2 + kind : 3 + kind, :] + modrow[kind : kind + 1, :]
            dst[at, :] = v.astype(BF16)

    hid_lat = hid.at[pl.ds(0, tokens)]
    hid_ctx = hid.at[pl.ds(tokens, n_ctx)]
    before = (me == G - 1) & (g < far - 1)
    after = (me == 0) & (g > 0)
    below = pl.ds(0, (WIN_ROWS // 2 - 1) * GRID_W)

    def slot(n):
        return pl.ds(pl.multiple_of(n * tokens, tokens), tokens)

    hidden(lat, hid_lat, tokens, 0)
    for i in range(2 * cols // TILE):
        tile = dot(hid_lat[...], wall[:, i * TILE : (i + 1) * TILE]).astype(BF16)
        for k in range(TILE // 256):
            kv_out[i * (TILE // 256) + k] = tile[:, k * 256 : (k + 1) * 256]
    for d in range(1, G):
        j = member(d)
        send(
            remote(
                kv_out.at[j],
                kv.at[slot(1 + me)],
                kv_send.at[d - 1],
                kv_recv.at[d - 1],
                {"sp": g * G + j},
            )
        )
    tile = dot(hid_lat[...], wall[:, 2 * cols : 3 * cols]).astype(BF16)
    for j in range(G):
        q_out[j] = tile[:, j * 128 : (j + 1) * 128]
    for d in range(1, G):
        j = member(d)
        send(
            remote(
                q_out.at[j],
                queries.at[me],
                q_send.at[d - 1],
                q_recv.at[d - 1],
                {"sp": g * G + j},
            )
        )
    for j in range(G):
        send(
            remote(
                kv_out.at[j],
                kv.at[slot(0)],
                h_send.at[j],
                h_recv.at[0],
                {"sp": lax.rem(g + 1, far) * G + j},
            ),
            before,
        )
        send(
            remote(
                kv_out.at[j, below],
                kv.at[pl.ds((G + 1) * tokens, (WIN_ROWS // 2 - 1) * GRID_W)],
                h_send.at[G + j],
                h_recv.at[1],
                {"sp": lax.rem(g + far - 1, far) * G + j},
            ),
            after,
        )

    def ctx_slot(f, j):
        b = other(f) * G + j
        return pl.ds(pl.multiple_of(b * n_ctx, n_ctx), n_ctx)

    def ctx_project(f):
        hidden(ctx.at[f], hid_ctx, n_ctx, 1)
        for i in range(2 * cols // TILE):
            tile = dot(hid_ctx[...], wall[:, i * TILE : (i + 1) * TILE]).astype(BF16)
            for k in range(TILE // 256):
                c_out[f, i * (TILE // 256) + k] = tile[:, k * 256 : (k + 1) * 256]
        for d in range(1, G):
            j = member(d)
            n = f * (G - 1) + d - 1
            send(
                remote(
                    c_out.at[f, j],
                    ckv.at[ctx_slot(f, me)],
                    c_send.at[n],
                    c_recv.at[n],
                    {"sp": g * G + j},
                )
            )

    ctx_project(0)
    kv[slot(1 + me), :] = kv_out[me]
    queries[me] = q_out[me]
    ckv[ctx_slot(0, me), :] = c_out[0, me]
    gate[...] = dot(hid_lat[...], wall[:, 3 * cols : 4 * cols]).astype(BF16)
    for f in range(1, far):
        ref = half_of(f, core)
        remote(ref, ref, f_send.at[f - 1], f_recv.at[f - 1], partner).wait_recv()
        send(remote(ref, ref, d_send.at[f - 1], d_recv.at[f - 1], partner))
    for f in range(1, far):
        ref = half_of(f, 1 - core)
        remote(ref, ref, d_send.at[f - 1], d_recv.at[f - 1], partner).wait_recv()
        ctx_project(f)
        ckv[ctx_slot(f, me), :] = c_out[f, me]

    for d in range(1, G):
        ref = kv.at[slot(1 + me)]
        remote(ref, ref, kv_send.at[d - 1], kv_recv.at[d - 1], partner).wait_recv()

    @pl.when(g > 0)
    def _():
        ref = kv.at[slot(0)]
        remote(ref, ref, h_send.at[0], h_recv.at[0], partner).wait_recv()

    @pl.when(g < far - 1)
    def _():
        ref = kv.at[pl.ds((G + 1) * tokens, (WIN_ROWS // 2 - 1) * GRID_W)]
        remote(ref, ref, h_send.at[G], h_recv.at[1], partner).wait_recv()

    for f in range(far):
        for d in range(1, G):
            n = f * (G - 1) + d - 1
            ref = ckv.at[ctx_slot(f, lax.rem(me + G - d, G))]
            remote(ref, ref, c_send.at[n], c_recv.at[n], partner).wait_recv()
    for d in range(1, G):
        ref = queries.at[lax.rem(me + G - d, G)]
        remote(ref, ref, q_send.at[d - 1], q_recv.at[d - 1], partner).wait_recv()

    total_rows = rows * S
    band_rows = rows // X
    span = band_rows * GRID_W
    half = lax.broadcasted_iota(jnp.int32, (span, 128), 1) < 64
    scale = 0.125

    def token_rows(x):
        return pl.ds(pl.multiple_of(x * span, span), span)

    def attend(phase, x, first, last):
        @pl.loop(first, last)
        def _(d):
            b = lax.rem(me + 1 + d, G)
            q2 = queries[b, token_rows(x), :].astype(F32) * scale
            outs = []
            for e in range(2):
                q = jnp.where(half if e == 0 else jnp.logical_not(half), q2, 0.0).astype(BF16)
                sc = dot_t(q, ckv[:, 0:128])
                sw = []
                bands = []
                for r in range(band_rows):
                    row = (g * G + b) * rows + x * band_rows + r
                    rs = jnp.clip(row - WIN_ROWS // 2, 0, total_rows - WIN_ROWS)
                    band = pl.ds(
                        pl.multiple_of((rs - g * G * rows + rows) * GRID_W, GRID_W),
                        WIN_ROWS * GRID_W,
                    )
                    bands.append(band)
                    offsets = jnp.concatenate(
                        [
                            table[e, rs - row + WIN_ROWS - 1 + 2 * p]
                            for p in range(WIN_ROWS // 2)
                        ],
                        axis=1,
                    )
                    sw.append(dot_t(q[r * GRID_W : (r + 1) * GRID_W], kv[band, 0:128]) + offsets)
                sw = jnp.concatenate(sw, axis=0)
                m = jnp.maximum(
                    jnp.max(sc, axis=-1, keepdims=True), jnp.max(sw, axis=-1, keepdims=True)
                )
                pc = jnp.exp(sc - m)
                pw = jnp.exp(sw - m)
                total = jnp.sum(pc, axis=-1, keepdims=True) + jnp.sum(pw, axis=-1, keepdims=True)
                pw = pw.astype(BF16)
                o = dot(pc.astype(BF16), ckv[:, 128:256])
                ow = [
                    dot(pw[r * GRID_W : (r + 1) * GRID_W], kv[bands[r], 128:256])
                    for r in range(band_rows)
                ]
                outs.append((o + jnp.concatenate(ow, axis=0)) / total)
            att_out[b, token_rows(x), :] = jnp.where(half, outs[0], outs[1]).astype(BF16)

            @pl.when(d < G - 1)
            def _():
                give_back(phase, x, d).start()

    def give_back(phase, x, d):
        b = lax.rem(me + 1 + d, G)
        n = phase * G + d
        return remote(
            att_out.at[b, token_rows(x)],
            att.at[me, token_rows(x)],
            o_send.at[n],
            o_recv.at[n],
            {"sp": g * G + b},
        )

    own = tokens // T
    piece = width // GROUPS

    def project_out(phase, x):
        att[me, token_rows(x), :] = att_out[me, token_rows(x), :]
        for d in range(G - 1):
            give_back(phase, x, d).wait()
        for j in range(G):
            at = slice(j * 128, (j + 1) * 128)
            a = gate[token_rows(x), at].astype(F32)
            a = a / (1.0 + jnp.exp(-a)) * att[j, token_rows(x), :].astype(F32)
            gate[token_rows(x), at] = a.astype(BF16)
        copies = []
        for n in range(GROUPS):
            at = pl.ds(n * piece, piece)
            prod[phase, :, at] = dot(gate[token_rows(x), :], wo[:, at]).astype(BF16)
            copy = remote(
                prod.at[phase, pl.ds(pl.multiple_of((1 - core) * own, own), own), at],
                mate.at[phase, :, at],
                m_send.at[phase * GROUPS + n],
                m_recv.at[phase * GROUPS + n],
                partner,
            )
            copy.start()
            copies.append(copy)
        return copies

    mine = pl.ds(pl.multiple_of(core * own, own), own)

    def cross_send(phase, x, copies):
        crossing = []
        for n in range(GROUPS):
            at = pl.ds(n * piece, piece)
            copies[n].wait()
            both = prod[phase, mine, at].astype(F32) + mate[phase, :, at].astype(F32)
            cross[phase, :, at] = both.astype(BF16)
            copy = remote(
                cross.at[phase, :, at],
                terms.at[phase, :, at],
                r_send.at[phase * GROUPS + n],
                r_recv.at[phase * GROUPS + n],
                {"tp": x * 2 + core},
            )
            copy.start()
            crossing.append(copy)
        return crossing

    crossing = []
    for phase in range(X):
        x = lax.rem(xi + phase + 1, X)
        attend(phase, x, 0, G)
        copies = project_out(phase, x)
        if phase < X - 1:
            crossing.append(cross_send(phase, x, copies))
    for n in range(GROUPS):
        at = pl.ds(n * piece, piece)
        copies[n].wait()
        total = prod[X - 1, mine, at].astype(F32) + mate[X - 1, :, at].astype(F32)
        for phase in range(X - 1):
            crossing[phase][n].wait()
            total = total + terms[phase, :, at].astype(F32)
        own_sum[:, at] = total.astype(BF16).astype(F32)
    b = own_sum[...]
    inv = lax.rsqrt(jnp.mean(b * b, axis=-1, keepdims=True) + EPSILON)
    own_at = pl.ds(pl.multiple_of(t * own, own), own)
    out[...] = (
        lat[own_at, :].astype(F32) + modrow[4:5, :] * (b * inv * gain_post[...])
    ).astype(BF16)

    for cond, copy in pending:
        if cond is None:
            copy.wait_send()
        else:

            @pl.when(cond)
            def _(copy=copy):
                copy.wait_send()


def shards(
    S,
    T,
    latent,
    context,
    condition,
    context_condition,
    gain_pre,
    gain_post,
    w_shift,
    w_scale,
    w_gate,
    w_query,
    w_key,
    w_value,
    w_silu,
    offset_bias,
    w_out,
):
    in_rows, cols = w_shift.shape
    tokens, width = latent.shape
    n_ctx = context.shape[0]
    heads = offset_bias.shape[0]
    turned = jnp.transpose(offset_bias, (1, 0, 2))
    pairs = turned.shape[0] - 1
    own_rows = tokens // T
    vmem = pl.BlockSpec(memory_space=pltpu.VMEM)
    hbm = pl.BlockSpec(memory_space=pl.ANY)
    sem = pltpu.SemaphoreType.DMA
    X = T // 2
    G = heads // 2
    far = S // G
    return pl.pallas_call(
        functools.partial(kernel, S, T),
        out_shape=jax.ShapeDtypeStruct((own_rows, width), BF16),
        in_specs=[hbm] * 15,
        out_specs=vmem,
        scratch_shapes=[
            pltpu.VMEM((width,), BF16),
            pltpu.VMEM((width,), BF16),
            pltpu.VMEM((16, width), F32),
            pltpu.VMEM((1, width), F32),
            pltpu.VMEM((1, width), F32),
            pltpu.VMEM(turned.shape, F32),
            pltpu.VMEM((pairs, heads, 2 * GRID_W), F32),
            pltpu.VMEM((tokens, width), BF16),
            pltpu.VMEM((far, n_ctx, width), BF16),
            pltpu.VMEM((3, in_rows, cols), BF16),
            pltpu.VMEM((width, 4 * cols), BF16),
            pltpu.VMEM((cols, width), BF16),
            pltpu.VMEM((8, cols), F32),
            pltpu.VMEM((S, 8, cols), F32),
            pltpu.VMEM((T, 8, cols), F32),
            pltpu.VMEM((8, width), F32),
            pltpu.VMEM((tokens + n_ctx, width), BF16),
            pltpu.VMEM((G, tokens, 256), BF16),
            pltpu.VMEM((G, tokens, 128), BF16),
            pltpu.VMEM((far, G, n_ctx, 256), BF16),
            pltpu.VMEM(((G + 2) * tokens, 256), BF16),
            pltpu.VMEM((G, tokens, 128), BF16),
            pltpu.VMEM((S * n_ctx, 256), BF16),
            pltpu.VMEM((tokens, cols), BF16),
            pltpu.VMEM((2, pairs, GRID_W, 2 * GRID_W), F32),
            pltpu.VMEM((G, tokens, 128), BF16),
            pltpu.VMEM((G, tokens, 128), BF16),
            pltpu.VMEM((X, tokens // X, width), BF16),
            pltpu.VMEM((X, own_rows, width), BF16),
            pltpu.VMEM((own_rows, width), F32),
            pltpu.VMEM((max(X - 1, 1), own_rows, width), BF16),
            pltpu.VMEM((max(X - 1, 1), own_rows, width), BF16),
            sem((13 + 2 * G,)),
            sem((max(S - 1, 1),)),
            sem((max(S - 1, 1),)),
            sem((max(T - 1, 1),)),
            sem((max(T - 1, 1),)),
            sem((max(far - 1, 1),)),
            sem((max(far - 1, 1),)),
            sem((max(far - 1, 1),)),
            sem((max(far - 1, 1),)),
            sem((max(G - 1, 1),)),
            sem((max(G - 1, 1),)),
            sem((max(G - 1, 1),)),
            sem((max(G - 1, 1),)),
            sem((max(far * (G - 1), 1),)),
            sem((max(far * (G - 1), 1),)),
            sem((2 * G,)),
            sem((2,)),
            sem((X * G,)),
            sem((X * G,)),
            sem((X * GROUPS,)),
            sem((X * GROUPS,)),
            sem((max(X - 1, 1) * GROUPS,)),
            sem((max(X - 1, 1) * GROUPS,)),
        ],
        compiler_params=pltpu.CompilerParams(
            collective_id=0, has_side_effects=True, vmem_limit_bytes=60 * 1024 * 1024
        ),
    )(
        condition,
        context_condition,
        gain_pre.reshape(1, width),
        gain_post.reshape(1, width),
        turned,
        latent,
        context,
        w_shift,
        w_scale,
        w_gate,
        w_query,
        w_key,
        w_value,
        w_silu,
        w_out,
    )


def solution(mesh):
    in_specs = (
        P("sp", None),
        P("sp", None),
        P(),
        P(),
        P(),
        P(),
        P("sp", "tp"),
        P("sp", "tp"),
        P("sp", "tp"),
        P(None, "tp"),
        P(None, "tp"),
        P(None, "tp"),
        P(None, "tp"),
        P("tp", None, None),
        P("tp", None),
    )
    return jax.shard_map(
        functools.partial(shards, mesh.shape["sp"], mesh.shape["tp"]),
        mesh=mesh,
        in_specs=in_specs,
        out_specs=P(("sp", "tp"), None),
        check_vma=False,
    )
```

```python
import functools

import jax
import jax.numpy as jnp
from jax import lax
from jax.experimental import pallas as pl
from jax.experimental.pallas import tpu as pltpu
from jax.sharding import PartitionSpec as P

GRID_W = 64
WIN_ROWS = 8
WIN_COLS = 16
EPSILON = 1e-06
MASKED = -1e30
F32 = jnp.float32
BF16 = jnp.bfloat16
TILE = 512
GROUPS = 4


def remote(src, dst, send, recv, where):
    return pltpu.make_async_remote_copy(
        src_ref=src,
        dst_ref=dst,
        send_sem=send,
        recv_sem=recv,
        device_id=where,
        device_id_type=pl.DeviceIdType.MESH,
    )


def dot(a, b):
    return jnp.dot(a, b, preferred_element_type=F32)


def dot_t(a, b):
    return lax.dot_general(a, b, (((1,), (1,)), ((), ())), preferred_element_type=F32)


def kernel(
    S,
    T,
    cond_hbm,
    ctx_cond_hbm,
    gain_pre_hbm,
    gain_post_hbm,
    bias_hbm,
    latent_hbm,
    context_hbm,
    wsh_hbm,
    wsc_hbm,
    wga_hbm,
    wq_hbm,
    wk_hbm,
    wv_hbm,
    ws_hbm,
    wo_hbm,
    out,
    cond_raw,
    ctx_cond_raw,
    active,
    gain_pre,
    gain_post,
    bias,
    lines,
    lat,
    ctx,
    wmod,
    wall,
    wo,
    part,
    modbuf,
    modfull,
    modrow,
    hid,
    kv_out,
    q_out,
    c_out,
    kv,
    queries,
    ckv,
    gate,
    table,
    att_out,
    att,
    prod,
    mate,
    own_sum,
    cross,
    terms,
    load_sem,
    a_send,
    a_recv,
    b_send,
    b_recv,
    f_send,
    f_recv,
    fx_send,
    fx_recv,
    d_send,
    d_recv,
    kv_send,
    kv_recv,
    q_send,
    q_recv,
    c_send,
    c_recv,
    h_send,
    h_recv,
    o_send,
    o_recv,
    m_send,
    m_recv,
    r_send,
    r_recv,
):
    s = lax.axis_index("sp")
    t = lax.axis_index("tp")
    tokens, width = lat.shape
    n_ctx = hid.shape[0] - tokens
    cols = wo.shape[0]
    in_rows = wmod.shape[1]
    rows = tokens // GRID_W
    G = kv_out.shape[0]
    far = S // G
    X = T // 2
    xi = t // 2
    core = t % 2
    g = s // G
    me = s % G
    partner = {"tp": t + 1 - 2 * core}
    half_width = width // 2
    pairs = table.shape[1]

    def member(d):
        if G & (G - 1) == 0:
            return me + d - 2 * (me & d)
        return lax.rem(me + d, G)

    def member_back(d):
        if G & (G - 1) == 0:
            return member(d)
        return lax.rem(me + G - d, G)

    def other(f):
        return lax.rem(g + f, far)

    loads = []

    def load(src, dst):
        copy = pltpu.make_async_copy(src, dst, load_sem.at[len(loads)])
        copy.start()
        loads.append(copy)

    load(cond_hbm, cond_raw)
    load(ctx_cond_hbm, ctx_cond_raw)
    load(wsh_hbm, wmod.at[0])
    load(wsc_hbm, wmod.at[1])
    load(wga_hbm, wmod.at[2])
    load(context_hbm, ctx.at[0])
    load(latent_hbm, lat)
    load(bias_hbm, bias)
    load(gain_pre_hbm, gain_pre)
    load(gain_post_hbm, gain_post)
    for j in range(G):
        load(wk_hbm.at[:, pl.ds(j * 128, 128)], wall.at[:, pl.ds(j * 256, 128)])
        load(wv_hbm.at[:, pl.ds(j * 128, 128)], wall.at[:, pl.ds(j * 256 + 128, 128)])
    load(wq_hbm, wall.at[:, pl.ds(2 * cols, cols)])
    load(ws_hbm, wall.at[:, pl.ds(3 * cols, cols)])
    load(wo_hbm, wo)

    barrier = pltpu.get_barrier_semaphore()
    for d in range(1, S):
        pl.semaphore_signal(
            barrier, inc=1, device_id={"sp": lax.rem(s + d, S)}, device_id_type=pl.DeviceIdType.MESH
        )
    for d in range(1, T):
        pl.semaphore_signal(
            barrier, inc=1, device_id={"tp": lax.rem(t + d, T)}, device_id_type=pl.DeviceIdType.MESH
        )

    pending = []

    def send(copy, cond=None):
        pending.append((cond, copy))
        if cond is None:
            copy.start()
        else:

            @pl.when(cond)
            def _():
                copy.start()

    part[...] = jnp.zeros_like(part)
    loads[0].wait()
    loads[1].wait()
    which = lax.broadcasted_iota(jnp.int32, (16, width), 0)
    active[...] = jnp.where(
        which == 0,
        cond_raw[...].astype(F32).reshape(1, width),
        jnp.where(which == 1, ctx_cond_raw[...].astype(F32).reshape(1, width), 0.0),
    )
    if in_rows % 128 == 0:
        own_cond = active[:, pl.ds(pl.multiple_of(s * in_rows, in_rows), in_rows)]
    else:
        shift = lax.rem(width - s * in_rows, width)
        own_cond = pltpu.roll(active[...], shift, 1)[:, 0:in_rows]
    own_active = (own_cond / (1.0 + jnp.exp(-own_cond))).astype(BF16)
    for i in range(3):
        loads[2 + i].wait()
        part[2 * i : 2 * i + 2, :] = dot(own_active, wmod[i])[0:2]
    loads[5].wait()
    pl.semaphore_wait(barrier, S - 1 + T - 1)

    a_copies = []
    for d in range(1, S):
        copy = remote(
            part, modbuf.at[s], a_send.at[d - 1], a_recv.at[d - 1], {"sp": lax.rem(s + d, S)}
        )
        copy.start()
        a_copies.append(copy)

    quarter = width // T

    def part_of(f, x, c):
        at = pl.ds(pl.multiple_of((x * 2 + c) * quarter, quarter), quarter)
        return ctx.at[f, :, at]

    def ctx_cross():
        for f in range(1, far):
            ref = part_of(f, xi, core)
            remote(ref, ref, f_send.at[f - 1], f_recv.at[f - 1], partner).wait_recv()
            for d in range(1, X):
                n = (f - 1) * (X - 1) + d - 1
                send(
                    remote(
                        ref,
                        ref,
                        fx_send.at[n],
                        fx_recv.at[n],
                        {"tp": lax.rem(xi + d, X) * 2 + core},
                    )
                )
            n = (f - 1) * X
            send(remote(ref, ref, d_send.at[n], d_recv.at[n], partner))

    def ctx_pass():
        for f in range(1, far):
            for d in range(1, X):
                ref = part_of(f, lax.rem(xi + X - d, X), core)
                n = (f - 1) * (X - 1) + d - 1
                remote(ref, ref, fx_send.at[n], fx_recv.at[n], partner).wait_recv()
                n = (f - 1) * X + d
                send(remote(ref, ref, d_send.at[n], d_recv.at[n], partner))

    def ctx_arrive(f):
        for d in range(X):
            ref = part_of(f, lax.rem(xi + X - d, X), 1 - core)
            n = (f - 1) * X + d
            remote(ref, ref, d_send.at[n], d_recv.at[n], partner).wait_recv()

    lane = lax.broadcasted_iota(jnp.int32, (GRID_W, 2 * GRID_W), 1) % GRID_W
    row = lax.broadcasted_iota(jnp.int32, (GRID_W, 2 * GRID_W), 0)
    first = jnp.clip(row - WIN_COLS // 2, 0, GRID_W - WIN_COLS)
    inside = (lane >= first) & (lane < first + WIN_COLS)
    loads[7].wait()
    blank = jnp.zeros((bias.shape[1], GRID_W - bias.shape[2]), F32)
    for p in range(pairs):
        lines[p] = jnp.concatenate([bias[p], blank, bias[p + 1], blank], axis=1)
    for e in range(2):
        for p in range(pairs):
            line = jnp.broadcast_to(lines[p, pl.ds(2 * me + e, 1), :], (GRID_W, 2 * GRID_W))
            rolled = pltpu.roll(line, 2 * GRID_W - (WIN_COLS - 1), 1, stride=1, stride_axis=0)
            table[e, p] = jnp.where(inside, rolled, MASKED)

    modbuf[s] = part[...]
    for copy in a_copies:
        copy.wait()
    modfull[t] = jnp.sum(modbuf[...], axis=0)
    b_copies = []
    for d in range(1, T):
        copy = remote(
            modfull.at[t],
            modfull.at[t],
            b_send.at[d - 1],
            b_recv.at[d - 1],
            {"tp": lax.rem(t + d, T)},
        )
        copy.start()
        b_copies.append(copy)
    for f in range(1, far):
        send(
            remote(
                part_of(0, xi, core),
                part_of(far - f, xi, core),
                f_send.at[far - f - 1],
                f_recv.at[far - f - 1],
                {"sp": other(f) * G + me},
            )
        )
    for i in range(6, len(loads)):
        if i != 7:
            loads[i].wait()
    for copy in b_copies:
        copy.wait()
    for j in range(T):
        at = slice(j * cols, (j + 1) * cols)
        modrow[:, at] = modfull[j]
        modrow[2:4, at] = gain_pre[:, at] * (1.0 + modfull[j, 2:4])

    def hidden(src, dst, count, kind):
        step = 32

        @pl.loop(0, count // step, unroll=min(4, count // step))
        def _(i):
            at = pl.ds(pl.multiple_of(i * step, step), step)
            v = src[at, :].astype(F32)
            inv = lax.rsqrt(jnp.mean(v * v, axis=-1, keepdims=True) + EPSILON)
            v = v * inv * modrow[2 + kind : 3 + kind, :] + modrow[kind : kind + 1, :]
            dst[at, :] = v.astype(BF16)

    hid_lat = hid.at[pl.ds(0, tokens)]
    hid_ctx = hid.at[pl.ds(tokens, n_ctx)]

    def slot(n):
        return pl.ds(pl.multiple_of(n * tokens, tokens), tokens)

    hidden(lat, hid_lat, tokens, 0)
    for i in range(2 * cols // TILE):
        tile = dot(hid_lat[...], wall[:, i * TILE : (i + 1) * TILE]).astype(BF16)
        for k in range(TILE // 256):
            kv_out[i * (TILE // 256) + k] = tile[:, k * 256 : (k + 1) * 256]
    for d in range(1, G):
        j = member(d)
        send(
            remote(
                kv_out.at[j],
                kv.at[slot(1 + me)],
                kv_send.at[d - 1],
                kv_recv.at[d - 1],
                {"sp": g * G + j},
            )
        )
    ctx_cross()
    tile = dot(hid_lat[...], wall[:, 2 * cols : 3 * cols]).astype(BF16)
    for j in range(G):
        q_out[j] = tile[:, j * 128 : (j + 1) * 128]
    for d in range(1, G):
        j = member(d)
        send(
            remote(
                q_out.at[j],
                queries.at[me],
                q_send.at[d - 1],
                q_recv.at[d - 1],
                {"sp": g * G + j},
            )
        )
    def ctx_slot(f, j):
        b = other(f) * G + j
        return pl.ds(pl.multiple_of(b * n_ctx, n_ctx), n_ctx)

    def ctx_project(f):
        hidden(ctx.at[f], hid_ctx, n_ctx, 1)
        for i in range(2 * cols // TILE):
            tile = dot(hid_ctx[...], wall[:, i * TILE : (i + 1) * TILE]).astype(BF16)
            for k in range(TILE // 256):
                c_out[f, i * (TILE // 256) + k] = tile[:, k * 256 : (k + 1) * 256]
        for d in range(1, G):
            j = member(d)
            n = f * (G - 1) + d - 1
            send(
                remote(
                    c_out.at[f, j],
                    ckv.at[ctx_slot(f, me)],
                    c_send.at[n],
                    c_recv.at[n],
                    {"sp": g * G + j},
                )
            )

    ctx_project(0)
    ctx_pass()
    kv[slot(1 + me), :] = kv_out[me]
    queries[me] = q_out[me]
    ckv[ctx_slot(0, me), :] = c_out[0, me]
    gate[...] = dot(hid_lat[...], wall[:, 3 * cols : 4 * cols]).astype(BF16)
    for f in range(1, far):
        ctx_arrive(f)
        ctx_project(f)
        ckv[ctx_slot(f, me), :] = c_out[f, me]

    for d in range(1, G):
        ref = kv.at[slot(1 + me)]
        remote(ref, ref, kv_send.at[d - 1], kv_recv.at[d - 1], partner).wait_recv()
    low = (WIN_ROWS // 2 - 1) * GRID_W
    send(
        remote(
            kv.at[slot(G)],
            kv.at[slot(0)],
            h_send.at[0],
            h_recv.at[0],
            {"sp": lax.rem(s + G, S)},
        ),
        g < far - 1,
    )
    send(
        remote(
            kv.at[pl.ds(tokens, low)],
            kv.at[pl.ds((G + 1) * tokens, low)],
            h_send.at[1],
            h_recv.at[1],
            {"sp": lax.rem(s + S - G, S)},
        ),
        g > 0,
    )

    @pl.when(g > 0)
    def _():
        ref = kv.at[slot(0)]
        remote(ref, ref, h_send.at[0], h_recv.at[0], partner).wait_recv()

    @pl.when(g < far - 1)
    def _():
        ref = kv.at[pl.ds((G + 1) * tokens, low)]
        remote(ref, ref, h_send.at[1], h_recv.at[1], partner).wait_recv()

    for f in range(far):
        for d in range(1, G):
            n = f * (G - 1) + d - 1
            ref = ckv.at[ctx_slot(f, member_back(d))]
            remote(ref, ref, c_send.at[n], c_recv.at[n], partner).wait_recv()
    for d in range(1, G):
        ref = queries.at[member_back(d)]
        remote(ref, ref, q_send.at[d - 1], q_recv.at[d - 1], partner).wait_recv()

    total_rows = rows * S
    band_rows = rows // X
    span = band_rows * GRID_W
    half = lax.broadcasted_iota(jnp.int32, (span, 128), 1) < 64
    scale = 0.125

    def token_rows(x):
        return pl.ds(pl.multiple_of(x * span, span), span)

    def attend(phase, x, first, last):
        @pl.loop(first, last)
        def _(d):
            b = lax.rem(me + 1 + d, G)
            q2 = queries[b, token_rows(x), :].astype(F32) * scale
            outs = []
            for e in range(2):
                q = jnp.where(half if e == 0 else jnp.logical_not(half), q2, 0.0).astype(BF16)
                sc = dot_t(q, ckv[:, 0:128])
                sw = []
                bands = []
                for r in range(band_rows):
                    row = (g * G + b) * rows + x * band_rows + r
                    rs = jnp.clip(row - WIN_ROWS // 2, 0, total_rows - WIN_ROWS)
                    band = pl.ds(
                        pl.multiple_of((rs - g * G * rows + rows) * GRID_W, GRID_W),
                        WIN_ROWS * GRID_W,
                    )
                    bands.append(band)
                    offsets = jnp.concatenate(
                        [
                            table[e, rs - row + WIN_ROWS - 1 + 2 * p]
                            for p in range(WIN_ROWS // 2)
                        ],
                        axis=1,
                    )
                    sw.append(dot_t(q[r * GRID_W : (r + 1) * GRID_W], kv[band, 0:128]) + offsets)
                sw = jnp.concatenate(sw, axis=0)
                m = jnp.maximum(
                    jnp.max(sc, axis=-1, keepdims=True), jnp.max(sw, axis=-1, keepdims=True)
                )
                pc = jnp.exp(sc - m)
                pw = jnp.exp(sw - m)
                total = jnp.sum(pc, axis=-1, keepdims=True) + jnp.sum(pw, axis=-1, keepdims=True)
                pw = pw.astype(BF16)
                o = dot(pc.astype(BF16), ckv[:, 128:256])
                ow = [
                    dot(pw[r * GRID_W : (r + 1) * GRID_W], kv[bands[r], 128:256])
                    for r in range(band_rows)
                ]
                outs.append((o + jnp.concatenate(ow, axis=0)) / total)
            att_out[b, token_rows(x), :] = jnp.where(half, outs[0], outs[1]).astype(BF16)

            @pl.when(d < G - 1)
            def _():
                give_back(phase, x, d).start()

    def give_back(phase, x, d):
        b = lax.rem(me + 1 + d, G)
        n = phase * G + d
        return remote(
            att_out.at[b, token_rows(x)],
            att.at[me, token_rows(x)],
            o_send.at[n],
            o_recv.at[n],
            {"sp": g * G + b},
        )

    own = tokens // T
    piece = width // GROUPS

    def project_out(phase, x):
        att[me, token_rows(x), :] = att_out[me, token_rows(x), :]
        for d in range(G - 1):
            give_back(phase, x, d).wait()
        for j in range(G):
            at = slice(j * 128, (j + 1) * 128)
            a = gate[token_rows(x), at].astype(F32)
            a = a / (1.0 + jnp.exp(-a)) * att[j, token_rows(x), :].astype(F32)
            gate[token_rows(x), at] = a.astype(BF16)
        copies = []
        for n in range(GROUPS):
            at = pl.ds(n * piece, piece)
            prod[phase, :, at] = dot(gate[token_rows(x), :], wo[:, at]).astype(BF16)
            copy = remote(
                prod.at[phase, pl.ds(pl.multiple_of((1 - core) * own, own), own), at],
                mate.at[phase, :, at],
                m_send.at[phase * GROUPS + n],
                m_recv.at[phase * GROUPS + n],
                partner,
            )
            copy.start()
            copies.append(copy)
        return copies

    mine = pl.ds(pl.multiple_of(core * own, own), own)

    def cross_send(phase, x, copies):
        crossing = []
        for n in range(GROUPS):
            at = pl.ds(n * piece, piece)
            copies[n].wait()
            both = prod[phase, mine, at].astype(F32) + mate[phase, :, at].astype(F32)
            cross[phase, :, at] = both.astype(BF16)
            copy = remote(
                cross.at[phase, :, at],
                terms.at[phase, :, at],
                r_send.at[phase * GROUPS + n],
                r_recv.at[phase * GROUPS + n],
                {"tp": x * 2 + core},
            )
            copy.start()
            crossing.append(copy)
        return crossing

    crossing = []
    order = [lax.rem(xi + phase + 1, X) for phase in range(X)]
    attend(0, order[0], 0, G)
    for phase in range(1, X):
        x, ahead = order[phase], order[phase - 1]
        attend(phase, x, 0, 1)
        copies = project_out(phase - 1, ahead)
        attend(phase, x, 1, G - 1)
        crossing.append(cross_send(phase - 1, ahead, copies))
        attend(phase, x, G - 1, G)
    copies = project_out(X - 1, order[X - 1])
    for n in range(GROUPS):
        at = pl.ds(n * piece, piece)
        copies[n].wait()
        total = prod[X - 1, mine, at].astype(F32) + mate[X - 1, :, at].astype(F32)
        for phase in range(X - 1):
            crossing[phase][n].wait()
            total = total + terms[phase, :, at].astype(F32)
        own_sum[:, at] = total.astype(BF16).astype(F32)
    b = own_sum[...]
    inv = lax.rsqrt(jnp.mean(b * b, axis=-1, keepdims=True) + EPSILON)
    own_at = pl.ds(pl.multiple_of(t * own, own), own)
    out[...] = (
        lat[own_at, :].astype(F32) + modrow[4:5, :] * (b * inv * gain_post[...])
    ).astype(BF16)

    for cond, copy in pending:
        if cond is None:
            copy.wait_send()
        else:

            @pl.when(cond)
            def _(copy=copy):
                copy.wait_send()


def shards(
    S,
    T,
    latent,
    context,
    condition,
    context_condition,
    gain_pre,
    gain_post,
    w_shift,
    w_scale,
    w_gate,
    w_query,
    w_key,
    w_value,
    w_silu,
    offset_bias,
    w_out,
):
    in_rows, cols = w_shift.shape
    tokens, width = latent.shape
    n_ctx = context.shape[0]
    heads = offset_bias.shape[0]
    turned = jnp.transpose(offset_bias, (1, 0, 2))
    pairs = turned.shape[0] - 1
    own_rows = tokens // T
    vmem = pl.BlockSpec(memory_space=pltpu.VMEM)
    hbm = pl.BlockSpec(memory_space=pl.ANY)
    sem = pltpu.SemaphoreType.DMA
    X = T // 2
    G = heads // 2
    far = S // G
    return pl.pallas_call(
        functools.partial(kernel, S, T),
        out_shape=jax.ShapeDtypeStruct((own_rows, width), BF16),
        in_specs=[hbm] * 15,
        out_specs=vmem,
        scratch_shapes=[
            pltpu.VMEM((width,), BF16),
            pltpu.VMEM((width,), BF16),
            pltpu.VMEM((16, width), F32),
            pltpu.VMEM((1, width), F32),
            pltpu.VMEM((1, width), F32),
            pltpu.VMEM(turned.shape, F32),
            pltpu.VMEM((pairs, heads, 2 * GRID_W), F32),
            pltpu.VMEM((tokens, width), BF16),
            pltpu.VMEM((far, n_ctx, width), BF16),
            pltpu.VMEM((3, in_rows, cols), BF16),
            pltpu.VMEM((width, 4 * cols), BF16),
            pltpu.VMEM((cols, width), BF16),
            pltpu.VMEM((8, cols), F32),
            pltpu.VMEM((S, 8, cols), F32),
            pltpu.VMEM((T, 8, cols), F32),
            pltpu.VMEM((8, width), F32),
            pltpu.VMEM((tokens + n_ctx, width), BF16),
            pltpu.VMEM((G, tokens, 256), BF16),
            pltpu.VMEM((G, tokens, 128), BF16),
            pltpu.VMEM((far, G, n_ctx, 256), BF16),
            pltpu.VMEM(((G + 2) * tokens, 256), BF16),
            pltpu.VMEM((G, tokens, 128), BF16),
            pltpu.VMEM((S * n_ctx, 256), BF16),
            pltpu.VMEM((tokens, cols), BF16),
            pltpu.VMEM((2, pairs, GRID_W, 2 * GRID_W), F32),
            pltpu.VMEM((G, tokens, 128), BF16),
            pltpu.VMEM((G, tokens, 128), BF16),
            pltpu.VMEM((X, tokens // X, width), BF16),
            pltpu.VMEM((X, own_rows, width), BF16),
            pltpu.VMEM((own_rows, width), F32),
            pltpu.VMEM((max(X - 1, 1), own_rows, width), BF16),
            pltpu.VMEM((max(X - 1, 1), own_rows, width), BF16),
            sem((13 + 2 * G,)),
            sem((max(S - 1, 1),)),
            sem((max(S - 1, 1),)),
            sem((max(T - 1, 1),)),
            sem((max(T - 1, 1),)),
            sem((max(far - 1, 1),)),
            sem((max(far - 1, 1),)),
            sem((max((far - 1) * (X - 1), 1),)),
            sem((max((far - 1) * (X - 1), 1),)),
            sem((max((far - 1) * X, 1),)),
            sem((max((far - 1) * X, 1),)),
            sem((max(G - 1, 1),)),
            sem((max(G - 1, 1),)),
            sem((max(G - 1, 1),)),
            sem((max(G - 1, 1),)),
            sem((max(far * (G - 1), 1),)),
            sem((max(far * (G - 1), 1),)),
            sem((2,)),
            sem((2,)),
            sem((X * G,)),
            sem((X * G,)),
            sem((X * GROUPS,)),
            sem((X * GROUPS,)),
            sem((max(X - 1, 1) * GROUPS,)),
            sem((max(X - 1, 1) * GROUPS,)),
        ],
        compiler_params=pltpu.CompilerParams(
            collective_id=0, has_side_effects=True, vmem_limit_bytes=60 * 1024 * 1024
        ),
    )(
        condition,
        context_condition,
        gain_pre.reshape(1, width),
        gain_post.reshape(1, width),
        turned,
        latent,
        context,
        w_shift,
        w_scale,
        w_gate,
        w_query,
        w_key,
        w_value,
        w_silu,
        w_out,
    )


def solution(mesh):
    in_specs = (
        P("sp", None),
        P("sp", None),
        P(),
        P(),
        P(),
        P(),
        P("sp", "tp"),
        P("sp", "tp"),
        P("sp", "tp"),
        P(None, "tp"),
        P(None, "tp"),
        P(None, "tp"),
        P(None, "tp"),
        P("tp", None, None),
        P("tp", None),
    )
    return jax.shard_map(
        functools.partial(shards, mesh.shape["sp"], mesh.shape["tp"]),
        mesh=mesh,
        in_specs=in_specs,
        out_specs=P(("sp", "tp"), None),
        check_vma=False,
    )
```

```python
import functools

import jax
import jax.numpy as jnp
from jax import lax
from jax.experimental import pallas as pl
from jax.experimental.pallas import tpu as pltpu
from jax.sharding import PartitionSpec as P

GRID_W = 64
WIN_ROWS = 8
WIN_COLS = 16
EPSILON = 1e-06
MASKED = -1e30
F32 = jnp.float32
BF16 = jnp.bfloat16
TILE = 512
GROUPS = 4
PIECES = 2


def remote(src, dst, send, recv, where):
    return pltpu.make_async_remote_copy(
        src_ref=src,
        dst_ref=dst,
        send_sem=send,
        recv_sem=recv,
        device_id=where,
        device_id_type=pl.DeviceIdType.MESH,
    )


def dot(a, b):
    return jnp.dot(a, b, preferred_element_type=F32)


def dot_t(a, b):
    return lax.dot_general(a, b, (((1,), (1,)), ((), ())), preferred_element_type=F32)


def kernel(
    S,
    T,
    cond_hbm,
    ctx_cond_hbm,
    gain_pre_hbm,
    gain_post_hbm,
    bias_hbm,
    latent_hbm,
    context_hbm,
    wsh_hbm,
    wsc_hbm,
    wga_hbm,
    wq_hbm,
    wk_hbm,
    wv_hbm,
    ws_hbm,
    wo_hbm,
    out,
    cond_raw,
    ctx_cond_raw,
    active,
    gain_pre,
    gain_post,
    bias,
    lines,
    lat,
    ctx,
    wmod,
    wall,
    wo,
    part,
    modbuf,
    modfull,
    modrow,
    hid,
    kv_out,
    q_out,
    c_out,
    kv,
    queries,
    ckv,
    gate,
    table,
    att_out,
    att,
    prod,
    mate,
    own_sum,
    cross,
    terms,
    load_sem,
    wave_sem,
    a_send,
    a_recv,
    b_send,
    b_recv,
    f_send,
    f_recv,
    fx_send,
    fx_recv,
    d_send,
    d_recv,
    g_send,
    g_recv,
    gm_send,
    gm_recv,
    kv_send,
    kv_recv,
    q_send,
    q_recv,
    c_send,
    c_recv,
    h_send,
    h_recv,
    o_send,
    o_recv,
    m_send,
    m_recv,
    r_send,
    r_recv,
):
    s = lax.axis_index("sp")
    t = lax.axis_index("tp")
    tokens = gate.shape[0]
    width = lat.shape[1]
    n_ctx = ctx.shape[1]
    cols = wo.shape[0]
    in_rows = wmod.shape[1]
    rows = tokens // GRID_W
    G = kv_out.shape[0]
    far = S // G
    X = T // 2
    xi = t // 2
    core = t % 2
    g = s // G
    me = s % G
    partner = {"tp": t + 1 - 2 * core}
    half_width = width // 2
    pairs = table.shape[1]
    halved = grid_halved(S, T, G)
    part_rows = tokens // 2
    own_first = part_rows if halved else 0

    def member(d):
        if G & (G - 1) == 0:
            return me + d - 2 * (me & d)
        return lax.rem(me + d, G)

    def member_back(d):
        if G & (G - 1) == 0:
            return member(d)
        return lax.rem(me + G - d, G)

    def other(f):
        return lax.rem(g + f, far)

    loads = []

    def load(src, dst):
        copy = pltpu.make_async_copy(src, dst, load_sem.at[len(loads)])
        copy.start()
        loads.append(copy)

    load(latent_hbm, lat.at[pl.ds(own_first, tokens)])
    load(cond_hbm, cond_raw)
    load(ctx_cond_hbm, ctx_cond_raw)
    load(wsh_hbm, wmod.at[0])
    load(wsc_hbm, wmod.at[1])
    load(wga_hbm, wmod.at[2])
    load(context_hbm, ctx.at[0])
    load(bias_hbm, bias)
    load(gain_pre_hbm, gain_pre)
    load(gain_post_hbm, gain_post)
    for j in range(G):
        load(wk_hbm.at[:, pl.ds(j * 128, 128)], wall.at[:, pl.ds(j * 256, 128)])
        load(wv_hbm.at[:, pl.ds(j * 128, 128)], wall.at[:, pl.ds(j * 256 + 128, 128)])
    load(wq_hbm, wall.at[:, pl.ds(2 * cols, cols)])
    load(ws_hbm, wall.at[:, pl.ds(3 * cols, cols)])
    load(wo_hbm, wo)

    _, Y, Z = layout_of(S, T)
    y = s % Y
    z = s // Y
    near = [(y < Y - 1, 1), (y > 0, S - 1), (z < Z - 1, Y), (z > 0, S - Y)]

    def greet(sem):
        for cond, step in near:

            @pl.when(cond)
            def _(step=step):
                pl.semaphore_signal(
                    sem,
                    inc=1,
                    device_id={"sp": lax.rem(s + step, S)},
                    device_id_type=pl.DeviceIdType.MESH,
                )

    n_near = sum(jnp.where(cond, 1, 0) for cond, _ in near)

    barrier = pltpu.get_barrier_semaphore()
    greet(barrier)
    for d in range(1, T):
        pl.semaphore_signal(
            barrier, inc=1, device_id={"tp": lax.rem(t + d, T)}, device_id_type=pl.DeviceIdType.MESH
        )

    pending = []

    def send(copy, cond=None):
        pending.append((cond, copy))
        if cond is None:
            copy.start()
        else:

            @pl.when(cond)
            def _():
                copy.start()

    def side_rows(k):
        return pl.ds(k * (own_first + tokens), part_rows)

    def side_of(k, c):
        return lat.at[
            side_rows(k), pl.ds(pl.multiple_of(c * half_width, half_width), half_width)
        ]

    def side_send(p):
        size = part_rows // PIECES
        at = pl.ds(pl.multiple_of(core * half_width, half_width), half_width)
        for k in range(2):
            first = k * (own_first + tokens) + p * size
            send(
                remote(
                    lat.at[pl.ds(own_first + k * part_rows + p * size, size), at],
                    lat.at[pl.ds(first, size), at],
                    g_send.at[k * PIECES + p],
                    g_recv.at[k * PIECES + p],
                    {"sp": g * G + member(k + 1)},
                )
            )

    def modulate():
        loads[1].wait()
        loads[2].wait()
        which = lax.broadcasted_iota(jnp.int32, (16, width), 0)
        active[...] = jnp.where(
            which == 0,
            cond_raw[...].astype(F32).reshape(1, width),
            jnp.where(which == 1, ctx_cond_raw[...].astype(F32).reshape(1, width), 0.0),
        )
        if in_rows % 128 == 0:
            own_cond = active[:, pl.ds(pl.multiple_of(s * in_rows, in_rows), in_rows)]
        else:
            shift = lax.rem(width - s * in_rows, width)
            own_cond = pltpu.roll(active[...], shift, 1)[:, 0:in_rows]
        own_active = (own_cond / (1.0 + jnp.exp(-own_cond))).astype(BF16)
        for i in range(3):
            loads[3 + i].wait()
            part[2 * i : 2 * i + 2, :] = dot(own_active, wmod[i])[0:2]

    part[...] = jnp.zeros_like(part)
    modulate()
    if halved:
        loads[0].wait()
    pl.semaphore_wait(barrier, n_near + T - 1)
    if halved:
        side_send(0)
    for w in range(Y + Z - 3):
        greet(wave_sem.at[w])
        pl.semaphore_wait(wave_sem.at[w], n_near)

    a_copies = []
    for d in range(1, S):
        copy = remote(
            part, modbuf.at[s], a_send.at[d - 1], a_recv.at[d - 1], {"sp": lax.rem(s + d, S)}
        )
        copy.start()
        a_copies.append(copy)

    quarter = width // T

    def part_of(f, x, c):
        at = pl.ds(pl.multiple_of((x * 2 + c) * quarter, quarter), quarter)
        return ctx.at[f, :, at]

    def ctx_cross():
        for f in range(1, far):
            ref = part_of(f, xi, core)
            remote(ref, ref, f_send.at[f - 1], f_recv.at[f - 1], partner).wait_recv()
            for d in range(1, X):
                n = (f - 1) * (X - 1) + d - 1
                send(
                    remote(
                        ref,
                        ref,
                        fx_send.at[n],
                        fx_recv.at[n],
                        {"tp": lax.rem(xi + d, X) * 2 + core},
                    )
                )
            n = (f - 1) * X
            send(remote(ref, ref, d_send.at[n], d_recv.at[n], partner))

    def ctx_pass():
        for f in range(1, far):
            for d in range(1, X):
                ref = part_of(f, lax.rem(xi + X - d, X), core)
                n = (f - 1) * (X - 1) + d - 1
                remote(ref, ref, fx_send.at[n], fx_recv.at[n], partner).wait_recv()
                n = (f - 1) * X + d
                send(remote(ref, ref, d_send.at[n], d_recv.at[n], partner))

    def ctx_arrive(f):
        for d in range(X):
            ref = part_of(f, lax.rem(xi + X - d, X), 1 - core)
            n = (f - 1) * X + d
            remote(ref, ref, d_send.at[n], d_recv.at[n], partner).wait_recv()

    if halved:
        for p in range(1, PIECES):
            side_send(p)

    lane = lax.broadcasted_iota(jnp.int32, (GRID_W, 2 * GRID_W), 1) % GRID_W
    row = lax.broadcasted_iota(jnp.int32, (GRID_W, 2 * GRID_W), 0)
    first = jnp.clip(row - WIN_COLS // 2, 0, GRID_W - WIN_COLS)
    inside = (lane >= first) & (lane < first + WIN_COLS)
    loads[7].wait()
    blank = jnp.zeros((bias.shape[1], GRID_W - bias.shape[2]), F32)
    for p in range(pairs):
        lines[p] = jnp.concatenate([bias[p], blank, bias[p + 1], blank], axis=1)
    for e in range(2):
        for p in range(pairs):
            line = jnp.broadcast_to(lines[p, pl.ds(2 * me + e, 1), :], (GRID_W, 2 * GRID_W))
            rolled = pltpu.roll(line, 2 * GRID_W - (WIN_COLS - 1), 1, stride=1, stride_axis=0)
            table[e, p] = jnp.where(inside, rolled, MASKED)

    modbuf[s] = part[...]
    for copy in a_copies:
        copy.wait()
    modfull[t] = jnp.sum(modbuf[...], axis=0)
    b_copies = []
    for d in range(1, T):
        copy = remote(
            modfull.at[t],
            modfull.at[t],
            b_send.at[d - 1],
            b_recv.at[d - 1],
            {"tp": lax.rem(t + d, T)},
        )
        copy.start()
        b_copies.append(copy)
    loads[6].wait()
    for f in range(1, far):
        send(
            remote(
                part_of(0, xi, core),
                part_of(far - f, xi, core),
                f_send.at[far - f - 1],
                f_recv.at[far - f - 1],
                {"sp": other(f) * G + me},
            )
        )
    if halved:
        size = part_rows // PIECES
        for k in range(2):
            for p in range(PIECES):
                at = pl.ds(pl.multiple_of(core * half_width, half_width), half_width)
                ref = lat.at[pl.ds(k * (own_first + tokens) + p * size, size), at]
                n = k * PIECES + p
                remote(ref, ref, g_send.at[n], g_recv.at[n], partner).wait_recv()
            ref = side_of(k, core)
            send(remote(ref, ref, gm_send.at[k], gm_recv.at[k], partner))
    for i in range(8, len(loads)):
        loads[i].wait()
    if not halved:
        loads[0].wait()
    for copy in b_copies:
        copy.wait()
    for j in range(T):
        at = slice(j * cols, (j + 1) * cols)
        modrow[:, at] = modfull[j]
        modrow[2:4, at] = gain_pre[:, at] * (1.0 + modfull[j, 2:4])

    def hidden(src, dst, count, kind):
        step = 32

        @pl.loop(0, count // step, unroll=min(4, count // step))
        def _(i):
            at = pl.ds(pl.multiple_of(i * step, step), step)
            v = src[at, :].astype(F32)
            inv = lax.rsqrt(jnp.mean(v * v, axis=-1, keepdims=True) + EPSILON)
            v = v * inv * modrow[2 + kind : 3 + kind, :] + modrow[kind : kind + 1, :]
            dst[at, :] = v.astype(BF16)

    own_rows = pl.ds(own_first, tokens)
    hid_ctx = hid.at[pl.ds(lat.shape[0], n_ctx)]

    def slot(n):
        return pl.ds(pl.multiple_of(n * tokens, tokens), tokens)

    def half_slot(n, k):
        return pl.ds(pl.multiple_of(n * tokens + k * part_rows, part_rows), part_rows)

    hidden(lat.at[own_rows], hid.at[own_rows], tokens, 0)
    kv_done = []
    q_done = []
    if halved:
        for k in range(2):
            ref = side_of(k, 1 - core)
            remote(ref, ref, gm_send.at[k], gm_recv.at[k], partner).wait_recv()
            hidden(lat.at[side_rows(k)], hid.at[side_rows(k)], part_rows, 0)
        sides = [
            (member(1), pl.ds(tokens, tokens), [(me, 1), (member(2), 1)]),
            (member(2), pl.ds(0, tokens), [(member(1), 0), (me, 0)]),
        ]

        def pair_dot(rows, j, first, size):
            at = pl.ds(pl.multiple_of(first + j * size, size), size)
            return dot(hid[rows, :], wall[:, at]).astype(BF16)

        def spread(first, size, staged, target, send_sems, recv_sems, done):
            for k, (j, rows, places) in enumerate(sides):
                staged[k] = pair_dot(rows, j, first, size)
                for n, (b, lower) in enumerate(places):
                    i = 2 * k + n
                    ref = target(b, lower)
                    copy = remote(
                        staged.at[k, pl.ds(n * part_rows, part_rows)],
                        ref,
                        send_sems.at[i],
                        recv_sems.at[i],
                        {"sp": g * G + j},
                    )
                    send(copy)
                    done.append(copy)

        def kv_part(b, k):
            return kv.at[half_slot(1 + b, k)]

        def q_part(b, k):
            return queries.at[b, pl.ds(k * part_rows, part_rows)]

        spread(0, 256, kv_out, kv_part, kv_send, kv_recv, kv_done)
        ctx_cross()
        spread(2 * cols, 128, q_out, q_part, q_send, q_recv, q_done)
    else:
        for i in range(2 * cols // TILE):
            tile = dot(hid[own_rows, :], wall[:, i * TILE : (i + 1) * TILE]).astype(BF16)
            for k in range(TILE // 256):
                kv_out[i * (TILE // 256) + k] = tile[:, k * 256 : (k + 1) * 256]
        for d in range(1, G):
            j = member(d)
            copy = remote(
                kv_out.at[j],
                kv.at[slot(1 + me)],
                kv_send.at[d - 1],
                kv_recv.at[d - 1],
                {"sp": g * G + j},
            )
            send(copy)
            kv_done.append(copy)
        ctx_cross()
        tile = dot(hid[own_rows, :], wall[:, 2 * cols : 3 * cols]).astype(BF16)
        for j in range(G):
            q_out[j] = tile[:, j * 128 : (j + 1) * 128]
        for d in range(1, G):
            j = member(d)
            copy = remote(
                q_out.at[j],
                queries.at[me],
                q_send.at[d - 1],
                q_recv.at[d - 1],
                {"sp": g * G + j},
            )
            send(copy)
            q_done.append(copy)

    def ctx_slot(f, j):
        b = other(f) * G + j
        return pl.ds(pl.multiple_of(b * n_ctx, n_ctx), n_ctx)

    def ctx_project(f):
        hidden(ctx.at[f], hid_ctx, n_ctx, 1)
        for i in range(2 * cols // TILE):
            tile = dot(hid_ctx[...], wall[:, i * TILE : (i + 1) * TILE]).astype(BF16)
            for k in range(TILE // 256):
                c_out[f, i * (TILE // 256) + k] = tile[:, k * 256 : (k + 1) * 256]
        for d in range(1, G):
            j = member(d)
            n = f * (G - 1) + d - 1
            send(
                remote(
                    c_out.at[f, j],
                    ckv.at[ctx_slot(f, me)],
                    c_send.at[n],
                    c_recv.at[n],
                    {"sp": g * G + j},
                )
            )

    ctx_project(0)
    ctx_pass()
    if halved:
        tile = pair_dot(pl.ds(0, 2 * tokens), me, 0, 256)
        kv[half_slot(1 + member(1), 0), :] = tile[0:part_rows]
        kv[slot(1 + me), :] = tile[part_rows : part_rows + tokens]
        kv[half_slot(1 + member(2), 1), :] = tile[part_rows + tokens :]
        tile = pair_dot(pl.ds(0, 2 * tokens), me, 2 * cols, 128)
        queries[member(1), 0:part_rows, :] = tile[0:part_rows]
        queries[me] = tile[part_rows : part_rows + tokens]
        queries[member(2), part_rows:tokens, :] = tile[part_rows + tokens :]
    else:
        kv[slot(1 + me), :] = kv_out[me]
        queries[me] = q_out[me]
    ckv[ctx_slot(0, me), :] = c_out[0, me]
    gate[...] = dot(hid[own_rows, :], wall[:, 3 * cols : 4 * cols]).astype(BF16)
    for f in range(1, far):
        ctx_arrive(f)
        ctx_project(f)
        ckv[ctx_slot(f, me), :] = c_out[f, me]

    for copy in kv_done:
        copy.wait_recv()
    low = (WIN_ROWS // 2 - 1) * GRID_W
    send(
        remote(
            kv.at[slot(G)],
            kv.at[slot(0)],
            h_send.at[0],
            h_recv.at[0],
            {"sp": lax.rem(s + G, S)},
        ),
        g < far - 1,
    )
    send(
        remote(
            kv.at[pl.ds(tokens, low)],
            kv.at[pl.ds((G + 1) * tokens, low)],
            h_send.at[1],
            h_recv.at[1],
            {"sp": lax.rem(s + S - G, S)},
        ),
        g > 0,
    )

    @pl.when(g > 0)
    def _():
        ref = kv.at[slot(0)]
        remote(ref, ref, h_send.at[0], h_recv.at[0], partner).wait_recv()

    @pl.when(g < far - 1)
    def _():
        ref = kv.at[pl.ds((G + 1) * tokens, low)]
        remote(ref, ref, h_send.at[1], h_recv.at[1], partner).wait_recv()

    for f in range(far):
        for d in range(1, G):
            n = f * (G - 1) + d - 1
            ref = ckv.at[ctx_slot(f, member_back(d))]
            remote(ref, ref, c_send.at[n], c_recv.at[n], partner).wait_recv()
    for copy in q_done:
        copy.wait_recv()

    total_rows = rows * S
    band_rows = rows // X
    span = band_rows * GRID_W
    half = lax.broadcasted_iota(jnp.int32, (span, 128), 1) < 64
    scale = 0.125

    def token_rows(x):
        return pl.ds(pl.multiple_of(x * span, span), span)

    def attend(phase, x, first, last):
        @pl.loop(first, last)
        def _(d):
            b = lax.rem(me + 1 + d, G)
            q2 = queries[b, token_rows(x), :].astype(F32) * scale
            outs = []
            for e in range(2):
                q = jnp.where(half if e == 0 else jnp.logical_not(half), q2, 0.0).astype(BF16)
                sc = dot_t(q, ckv[:, 0:128])
                sw = []
                bands = []
                for r in range(band_rows):
                    row = (g * G + b) * rows + x * band_rows + r
                    rs = jnp.clip(row - WIN_ROWS // 2, 0, total_rows - WIN_ROWS)
                    band = pl.ds(
                        pl.multiple_of((rs - g * G * rows + rows) * GRID_W, GRID_W),
                        WIN_ROWS * GRID_W,
                    )
                    bands.append(band)
                    offsets = jnp.concatenate(
                        [
                            table[e, rs - row + WIN_ROWS - 1 + 2 * p]
                            for p in range(WIN_ROWS // 2)
                        ],
                        axis=1,
                    )
                    sw.append(dot_t(q[r * GRID_W : (r + 1) * GRID_W], kv[band, 0:128]) + offsets)
                sw = jnp.concatenate(sw, axis=0)
                m = jnp.maximum(
                    jnp.max(sc, axis=-1, keepdims=True), jnp.max(sw, axis=-1, keepdims=True)
                )
                pc = jnp.exp(sc - m)
                pw = jnp.exp(sw - m)
                total = jnp.sum(pc, axis=-1, keepdims=True) + jnp.sum(pw, axis=-1, keepdims=True)
                pw = pw.astype(BF16)
                o = dot(pc.astype(BF16), ckv[:, 128:256])
                ow = [
                    dot(pw[r * GRID_W : (r + 1) * GRID_W], kv[bands[r], 128:256])
                    for r in range(band_rows)
                ]
                outs.append((o + jnp.concatenate(ow, axis=0)) / total)
            att_out[b, token_rows(x), :] = jnp.where(half, outs[0], outs[1]).astype(BF16)

            @pl.when(d < G - 1)
            def _():
                give_back(phase, x, d).start()

    def give_back(phase, x, d):
        b = lax.rem(me + 1 + d, G)
        n = phase * G + d
        return remote(
            att_out.at[b, token_rows(x)],
            att.at[me, token_rows(x)],
            o_send.at[n],
            o_recv.at[n],
            {"sp": g * G + b},
        )

    own = tokens // T
    piece = width // GROUPS

    def project_out(phase, x):
        att[me, token_rows(x), :] = att_out[me, token_rows(x), :]
        for d in range(G - 1):
            give_back(phase, x, d).wait()
        for j in range(G):
            at = slice(j * 128, (j + 1) * 128)
            a = gate[token_rows(x), at].astype(F32)
            a = a / (1.0 + jnp.exp(-a)) * att[j, token_rows(x), :].astype(F32)
            gate[token_rows(x), at] = a.astype(BF16)
        copies = []
        for n in range(GROUPS):
            at = pl.ds(n * piece, piece)
            prod[phase, :, at] = dot(gate[token_rows(x), :], wo[:, at]).astype(BF16)
            copy = remote(
                prod.at[phase, pl.ds(pl.multiple_of((1 - core) * own, own), own), at],
                mate.at[phase, :, at],
                m_send.at[phase * GROUPS + n],
                m_recv.at[phase * GROUPS + n],
                partner,
            )
            copy.start()
            copies.append(copy)
        return copies

    mine = pl.ds(pl.multiple_of(core * own, own), own)

    def cross_send(phase, x, copies):
        crossing = []
        for n in range(GROUPS):
            at = pl.ds(n * piece, piece)
            copies[n].wait()
            both = prod[phase, mine, at].astype(F32) + mate[phase, :, at].astype(F32)
            cross[phase, :, at] = both.astype(BF16)
            copy = remote(
                cross.at[phase, :, at],
                terms.at[phase, :, at],
                r_send.at[phase * GROUPS + n],
                r_recv.at[phase * GROUPS + n],
                {"tp": x * 2 + core},
            )
            copy.start()
            crossing.append(copy)
        return crossing

    crossing = []
    order = [lax.rem(xi + phase + 1, X) for phase in range(X)]
    attend(0, order[0], 0, G)
    for phase in range(1, X):
        x, ahead = order[phase], order[phase - 1]
        attend(phase, x, 0, 1)
        copies = project_out(phase - 1, ahead)
        attend(phase, x, 1, G - 1)
        crossing.append(cross_send(phase - 1, ahead, copies))
        attend(phase, x, G - 1, G)
    copies = project_out(X - 1, order[X - 1])
    for n in range(GROUPS):
        at = pl.ds(n * piece, piece)
        copies[n].wait()
        total = prod[X - 1, mine, at].astype(F32) + mate[X - 1, :, at].astype(F32)
        for phase in range(X - 1):
            crossing[phase][n].wait()
            total = total + terms[phase, :, at].astype(F32)
        own_sum[:, at] = total.astype(BF16).astype(F32)
    b = own_sum[...]
    inv = lax.rsqrt(jnp.mean(b * b, axis=-1, keepdims=True) + EPSILON)
    own_at = pl.ds(pl.multiple_of(own_first + t * own, own), own)
    out[...] = (
        lat[own_at, :].astype(F32) + modrow[4:5, :] * (b * inv * gain_post[...])
    ).astype(BF16)

    for cond, copy in pending:
        if cond is None:
            copy.wait_send()
        else:

            @pl.when(cond)
            def _(copy=copy):
                copy.wait_send()


def layout_of(S, T):
    X = T // 2
    Y = X if S % X == 0 else 1
    return X, Y, S // Y


def grid_halved(S, T, G):
    return G == 4 and layout_of(S, T)[1] == 2


def shards(
    S,
    T,
    latent,
    context,
    condition,
    context_condition,
    gain_pre,
    gain_post,
    w_shift,
    w_scale,
    w_gate,
    w_query,
    w_key,
    w_value,
    w_silu,
    offset_bias,
    w_out,
):
    in_rows, cols = w_shift.shape
    tokens, width = latent.shape
    n_ctx = context.shape[0]
    heads = offset_bias.shape[0]
    turned = jnp.transpose(offset_bias, (1, 0, 2))
    pairs = turned.shape[0] - 1
    own_rows = tokens // T
    vmem = pl.BlockSpec(memory_space=pltpu.VMEM)
    hbm = pl.BlockSpec(memory_space=pl.ANY)
    sem = pltpu.SemaphoreType.DMA
    X = T // 2
    G = heads // 2
    far = S // G
    held = 2 * tokens if grid_halved(S, T, G) else tokens
    _, Y, Z = layout_of(S, T)
    return pl.pallas_call(
        functools.partial(kernel, S, T),
        out_shape=jax.ShapeDtypeStruct((own_rows, width), BF16),
        in_specs=[hbm] * 15,
        out_specs=vmem,
        scratch_shapes=[
            pltpu.VMEM((width,), BF16),
            pltpu.VMEM((width,), BF16),
            pltpu.VMEM((16, width), F32),
            pltpu.VMEM((1, width), F32),
            pltpu.VMEM((1, width), F32),
            pltpu.VMEM(turned.shape, F32),
            pltpu.VMEM((pairs, heads, 2 * GRID_W), F32),
            pltpu.VMEM((held, width), BF16),
            pltpu.VMEM((far, n_ctx, width), BF16),
            pltpu.VMEM((3, in_rows, cols), BF16),
            pltpu.VMEM((width, 4 * cols), BF16),
            pltpu.VMEM((cols, width), BF16),
            pltpu.VMEM((8, cols), F32),
            pltpu.VMEM((S, 8, cols), F32),
            pltpu.VMEM((T, 8, cols), F32),
            pltpu.VMEM((8, width), F32),
            pltpu.VMEM((held + n_ctx, width), BF16),
            pltpu.VMEM((G, tokens, 256), BF16),
            pltpu.VMEM((G, tokens, 128), BF16),
            pltpu.VMEM((far, G, n_ctx, 256), BF16),
            pltpu.VMEM(((G + 2) * tokens, 256), BF16),
            pltpu.VMEM((G, tokens, 128), BF16),
            pltpu.VMEM((S * n_ctx, 256), BF16),
            pltpu.VMEM((tokens, cols), BF16),
            pltpu.VMEM((2, pairs, GRID_W, 2 * GRID_W), F32),
            pltpu.VMEM((G, tokens, 128), BF16),
            pltpu.VMEM((G, tokens, 128), BF16),
            pltpu.VMEM((X, tokens // X, width), BF16),
            pltpu.VMEM((X, own_rows, width), BF16),
            pltpu.VMEM((own_rows, width), F32),
            pltpu.VMEM((max(X - 1, 1), own_rows, width), BF16),
            pltpu.VMEM((max(X - 1, 1), own_rows, width), BF16),
            sem((13 + 2 * G,)),
            pltpu.SemaphoreType.REGULAR((max(Y + Z - 3, 1),)),
            sem((max(S - 1, 1),)),
            sem((max(S - 1, 1),)),
            sem((max(T - 1, 1),)),
            sem((max(T - 1, 1),)),
            sem((max(far - 1, 1),)),
            sem((max(far - 1, 1),)),
            sem((max((far - 1) * (X - 1), 1),)),
            sem((max((far - 1) * (X - 1), 1),)),
            sem((max((far - 1) * X, 1),)),
            sem((max((far - 1) * X, 1),)),
            sem((2 * PIECES,)),
            sem((2 * PIECES,)),
            sem((2,)),
            sem((2,)),
            sem((G,)),
            sem((G,)),
            sem((G,)),
            sem((G,)),
            sem((max(far * (G - 1), 1),)),
            sem((max(far * (G - 1), 1),)),
            sem((2,)),
            sem((2,)),
            sem((X * G,)),
            sem((X * G,)),
            sem((X * GROUPS,)),
            sem((X * GROUPS,)),
            sem((max(X - 1, 1) * GROUPS,)),
            sem((max(X - 1, 1) * GROUPS,)),
        ],
        compiler_params=pltpu.CompilerParams(
            collective_id=0, has_side_effects=True, vmem_limit_bytes=60 * 1024 * 1024
        ),
    )(
        condition,
        context_condition,
        gain_pre.reshape(1, width),
        gain_post.reshape(1, width),
        turned,
        latent,
        context,
        w_shift,
        w_scale,
        w_gate,
        w_query,
        w_key,
        w_value,
        w_silu,
        w_out,
    )


def solution(mesh):
    in_specs = (
        P("sp", None),
        P("sp", None),
        P(),
        P(),
        P(),
        P(),
        P("sp", "tp"),
        P("sp", "tp"),
        P("sp", "tp"),
        P(None, "tp"),
        P(None, "tp"),
        P(None, "tp"),
        P(None, "tp"),
        P("tp", None, None),
        P("tp", None),
    )
    return jax.shard_map(
        functools.partial(shards, mesh.shape["sp"], mesh.shape["tp"]),
        mesh=mesh,
        in_specs=in_specs,
        out_specs=P(("sp", "tp"), None),
        check_vma=False,
    )
```

```python
import functools

import jax
import jax.numpy as jnp
from jax import lax
from jax.experimental import pallas as pl
from jax.experimental.pallas import tpu as pltpu
from jax.sharding import PartitionSpec as P

GRID_W = 64
WIN_ROWS = 8
WIN_COLS = 16
EPSILON = 1e-06
MASKED = -1e30
F32 = jnp.float32
BF16 = jnp.bfloat16
TILE = 512
GROUPS = 2
PIECES = 2


def remote(src, dst, send, recv, where):
    return pltpu.make_async_remote_copy(
        src_ref=src,
        dst_ref=dst,
        send_sem=send,
        recv_sem=recv,
        device_id=where,
        device_id_type=pl.DeviceIdType.MESH,
    )


def dot(a, b):
    return jnp.dot(a, b, preferred_element_type=F32)


def dot_t(a, b):
    return lax.dot_general(a, b, (((1,), (1,)), ((), ())), preferred_element_type=F32)


def kernel(
    S,
    T,
    cond_hbm,
    ctx_cond_hbm,
    gain_pre_hbm,
    gain_post_hbm,
    bias_hbm,
    latent_hbm,
    context_hbm,
    wsh_hbm,
    wsc_hbm,
    wga_hbm,
    wq_hbm,
    wk_hbm,
    wv_hbm,
    ws_hbm,
    wo_hbm,
    out,
    cond_raw,
    ctx_cond_raw,
    active,
    gain_pre,
    gain_post,
    bias,
    lines,
    lat,
    ctx,
    wmod,
    wall,
    wo,
    part,
    modbuf,
    modfull,
    modrow,
    hid,
    kv_out,
    q_out,
    c_out,
    kv,
    queries,
    ckv,
    gate,
    table,
    att_out,
    att,
    prod,
    mate,
    own_sum,
    cross,
    terms,
    load_sem,
    wave_sem,
    a_send,
    a_recv,
    b_send,
    b_recv,
    f_send,
    f_recv,
    fx_send,
    fx_recv,
    d_send,
    d_recv,
    g_send,
    g_recv,
    gm_send,
    gm_recv,
    kv_send,
    kv_recv,
    q_send,
    q_recv,
    c_send,
    c_recv,
    h_send,
    h_recv,
    o_send,
    o_recv,
    m_send,
    m_recv,
    r_send,
    r_recv,
):
    s = lax.axis_index("sp")
    t = lax.axis_index("tp")
    tokens = gate.shape[0]
    width = lat.shape[1]
    n_ctx = ctx.shape[1]
    cols = wo.shape[0]
    in_rows = wmod.shape[1]
    rows = tokens // GRID_W
    G = kv_out.shape[0]
    far = S // G
    X = T // 2
    xi = t // 2
    core = t % 2
    g = s // G
    me = s % G
    partner = {"tp": t + 1 - 2 * core}
    half_width = width // 2
    pairs = table.shape[1]
    halved = grid_halved(S, T, G)
    part_rows = tokens // 2
    own_first = part_rows if halved else 0

    def member(d):
        if G & (G - 1) == 0:
            return me + d - 2 * (me & d)
        return lax.rem(me + d, G)

    def member_back(d):
        if G & (G - 1) == 0:
            return member(d)
        return lax.rem(me + G - d, G)

    def other(f):
        return lax.rem(g + f, far)

    loads = []

    def load(src, dst):
        copy = pltpu.make_async_copy(src, dst, load_sem.at[len(loads)])
        copy.start()
        loads.append(copy)

    load(latent_hbm, lat.at[pl.ds(own_first, tokens)])
    load(cond_hbm, cond_raw)
    load(ctx_cond_hbm, ctx_cond_raw)
    load(wsh_hbm, wmod.at[0])
    load(wsc_hbm, wmod.at[1])
    load(wga_hbm, wmod.at[2])
    load(context_hbm, ctx.at[0])
    load(bias_hbm, bias)
    load(gain_pre_hbm, gain_pre)
    load(gain_post_hbm, gain_post)
    for j in range(G):
        load(wk_hbm.at[:, pl.ds(j * 128, 128)], wall.at[:, pl.ds(j * 256, 128)])
        load(wv_hbm.at[:, pl.ds(j * 128, 128)], wall.at[:, pl.ds(j * 256 + 128, 128)])
    load(wq_hbm, wall.at[:, pl.ds(2 * cols, cols)])
    load(ws_hbm, wall.at[:, pl.ds(3 * cols, cols)])
    load(wo_hbm, wo)

    _, Y, Z = layout_of(S, T)
    y = s % Y
    z = s // Y
    near = [(y < Y - 1, 1), (y > 0, S - 1), (z < Z - 1, Y), (z > 0, S - Y)]

    def greet(sem):
        for cond, step in near:

            @pl.when(cond)
            def _(step=step):
                pl.semaphore_signal(
                    sem,
                    inc=1,
                    device_id={"sp": lax.rem(s + step, S)},
                    device_id_type=pl.DeviceIdType.MESH,
                )

    n_near = sum(jnp.where(cond, 1, 0) for cond, _ in near)

    barrier = pltpu.get_barrier_semaphore()
    greet(barrier)
    for d in range(1, T):
        pl.semaphore_signal(
            barrier, inc=1, device_id={"tp": lax.rem(t + d, T)}, device_id_type=pl.DeviceIdType.MESH
        )

    pending = []

    def send(copy, cond=None):
        pending.append((cond, copy))
        if cond is None:
            copy.start()
        else:

            @pl.when(cond)
            def _():
                copy.start()

    def side_rows(k):
        return pl.ds(k * (own_first + tokens), part_rows)

    def side_of(k, c):
        return lat.at[
            side_rows(k), pl.ds(pl.multiple_of(c * half_width, half_width), half_width)
        ]

    def side_send(p):
        size = part_rows // PIECES
        at = pl.ds(pl.multiple_of(core * half_width, half_width), half_width)
        for k in range(2):
            first = k * (own_first + tokens) + p * size
            send(
                remote(
                    lat.at[pl.ds(own_first + k * part_rows + p * size, size), at],
                    lat.at[pl.ds(first, size), at],
                    g_send.at[k * PIECES + p],
                    g_recv.at[k * PIECES + p],
                    {"sp": g * G + member(k + 1)},
                )
            )

    def modulate():
        loads[1].wait()
        loads[2].wait()
        which = lax.broadcasted_iota(jnp.int32, (16, width), 0)
        active[...] = jnp.where(
            which == 0,
            cond_raw[...].astype(F32).reshape(1, width),
            jnp.where(which == 1, ctx_cond_raw[...].astype(F32).reshape(1, width), 0.0),
        )
        if in_rows % 128 == 0:
            own_cond = active[:, pl.ds(pl.multiple_of(s * in_rows, in_rows), in_rows)]
        else:
            shift = lax.rem(width - s * in_rows, width)
            own_cond = pltpu.roll(active[...], shift, 1)[:, 0:in_rows]
        own_active = (own_cond / (1.0 + jnp.exp(-own_cond))).astype(BF16)
        for i in range(3):
            loads[3 + i].wait()
            part[2 * i : 2 * i + 2, :] = dot(own_active, wmod[i])[0:2]

    part[...] = jnp.zeros_like(part)
    modulate()
    if halved:
        loads[0].wait()
    pl.semaphore_wait(barrier, n_near + T - 1)
    if halved:
        side_send(0)
    for w in range(Y + Z - 3):
        greet(wave_sem.at[w])
        pl.semaphore_wait(wave_sem.at[w], n_near)

    a_copies = []
    for d in range(1, S):
        copy = remote(
            part, modbuf.at[s], a_send.at[d - 1], a_recv.at[d - 1], {"sp": lax.rem(s + d, S)}
        )
        copy.start()
        a_copies.append(copy)

    quarter = width // T

    def part_of(f, x, c):
        at = pl.ds(pl.multiple_of((x * 2 + c) * quarter, quarter), quarter)
        return ctx.at[f, :, at]

    def ctx_cross():
        for f in range(1, far):
            ref = part_of(f, xi, core)
            remote(ref, ref, f_send.at[f - 1], f_recv.at[f - 1], partner).wait_recv()
            for d in range(1, X):
                n = (f - 1) * (X - 1) + d - 1
                send(
                    remote(
                        ref,
                        ref,
                        fx_send.at[n],
                        fx_recv.at[n],
                        {"tp": lax.rem(xi + d, X) * 2 + core},
                    )
                )
            n = (f - 1) * X
            send(remote(ref, ref, d_send.at[n], d_recv.at[n], partner))

    def ctx_pass():
        for f in range(1, far):
            for d in range(1, X):
                ref = part_of(f, lax.rem(xi + X - d, X), core)
                n = (f - 1) * (X - 1) + d - 1
                remote(ref, ref, fx_send.at[n], fx_recv.at[n], partner).wait_recv()
                n = (f - 1) * X + d
                send(remote(ref, ref, d_send.at[n], d_recv.at[n], partner))

    def ctx_arrive(f):
        for d in range(X):
            ref = part_of(f, lax.rem(xi + X - d, X), 1 - core)
            n = (f - 1) * X + d
            remote(ref, ref, d_send.at[n], d_recv.at[n], partner).wait_recv()

    if halved:
        for p in range(1, PIECES):
            side_send(p)

    lane = lax.broadcasted_iota(jnp.int32, (GRID_W, 2 * GRID_W), 1) % GRID_W
    row = lax.broadcasted_iota(jnp.int32, (GRID_W, 2 * GRID_W), 0)
    first = jnp.clip(row - WIN_COLS // 2, 0, GRID_W - WIN_COLS)
    inside = (lane >= first) & (lane < first + WIN_COLS)
    loads[7].wait()
    blank = jnp.zeros((bias.shape[1], GRID_W - bias.shape[2]), F32)
    for p in range(pairs):
        lines[p] = jnp.concatenate([bias[p], blank, bias[p + 1], blank], axis=1)
    for e in range(2):
        for p in range(pairs):
            line = jnp.broadcast_to(lines[p, pl.ds(2 * me + e, 1), :], (GRID_W, 2 * GRID_W))
            rolled = pltpu.roll(line, 2 * GRID_W - (WIN_COLS - 1), 1, stride=1, stride_axis=0)
            table[e, p] = jnp.where(inside, rolled, MASKED)

    modbuf[s] = part[...]
    for copy in a_copies:
        copy.wait()
    modfull[t] = jnp.sum(modbuf[...], axis=0)
    b_copies = []
    for d in range(1, T):
        copy = remote(
            modfull.at[t],
            modfull.at[t],
            b_send.at[d - 1],
            b_recv.at[d - 1],
            {"tp": lax.rem(t + d, T)},
        )
        copy.start()
        b_copies.append(copy)
    loads[6].wait()
    for f in range(1, far):
        send(
            remote(
                part_of(0, xi, core),
                part_of(far - f, xi, core),
                f_send.at[far - f - 1],
                f_recv.at[far - f - 1],
                {"sp": other(f) * G + me},
            )
        )
    if halved:
        size = part_rows // PIECES
        for k in range(2):
            for p in range(PIECES):
                at = pl.ds(pl.multiple_of(core * half_width, half_width), half_width)
                ref = lat.at[pl.ds(k * (own_first + tokens) + p * size, size), at]
                n = k * PIECES + p
                remote(ref, ref, g_send.at[n], g_recv.at[n], partner).wait_recv()
            ref = side_of(k, core)
            send(remote(ref, ref, gm_send.at[k], gm_recv.at[k], partner))
    for i in range(8, len(loads)):
        loads[i].wait()
    if not halved:
        loads[0].wait()
    for copy in b_copies:
        copy.wait()
    for j in range(T):
        at = slice(j * cols, (j + 1) * cols)
        modrow[:, at] = modfull[j]
        modrow[2:4, at] = gain_pre[:, at] * (1.0 + modfull[j, 2:4])

    def hidden(src, dst, count, kind):
        step = 32

        @pl.loop(0, count // step, unroll=min(4, count // step))
        def _(i):
            at = pl.ds(pl.multiple_of(i * step, step), step)
            v = src[at, :].astype(F32)
            inv = lax.rsqrt(jnp.mean(v * v, axis=-1, keepdims=True) + EPSILON)
            v = v * inv * modrow[2 + kind : 3 + kind, :] + modrow[kind : kind + 1, :]
            dst[at, :] = v.astype(BF16)

    own_rows = pl.ds(own_first, tokens)
    hid_ctx = hid.at[pl.ds(lat.shape[0], n_ctx)]

    def slot(n):
        return pl.ds(pl.multiple_of(n * tokens, tokens), tokens)

    def half_slot(n, k):
        return pl.ds(pl.multiple_of(n * tokens + k * part_rows, part_rows), part_rows)

    hidden(lat.at[own_rows], hid.at[own_rows], tokens, 0)
    kv_done = []
    q_done = []
    if halved:
        for k in range(2):
            ref = side_of(k, 1 - core)
            remote(ref, ref, gm_send.at[k], gm_recv.at[k], partner).wait_recv()
            hidden(lat.at[side_rows(k)], hid.at[side_rows(k)], part_rows, 0)
        sides = [
            (member(1), pl.ds(tokens, tokens), [(me, 1), (member(2), 1)]),
            (member(2), pl.ds(0, tokens), [(member(1), 0), (me, 0)]),
        ]

        def pair_dot(rows, j, first, size):
            at = pl.ds(pl.multiple_of(first + j * size, size), size)
            return dot(hid[rows, :], wall[:, at]).astype(BF16)

        def spread(first, size, staged, target, send_sems, recv_sems, done):
            for k, (j, rows, places) in enumerate(sides):
                staged[k] = pair_dot(rows, j, first, size)
                for n, (b, lower) in enumerate(places):
                    i = 2 * k + n
                    ref = target(b, lower)
                    copy = remote(
                        staged.at[k, pl.ds(n * part_rows, part_rows)],
                        ref,
                        send_sems.at[i],
                        recv_sems.at[i],
                        {"sp": g * G + j},
                    )
                    send(copy)
                    done.append(copy)

        def kv_part(b, k):
            return kv.at[half_slot(1 + b, k)]

        def q_part(b, k):
            return queries.at[b, pl.ds(k * part_rows, part_rows)]

        spread(0, 256, kv_out, kv_part, kv_send, kv_recv, kv_done)
        ctx_cross()
        spread(2 * cols, 128, q_out, q_part, q_send, q_recv, q_done)
    else:
        for i in range(2 * cols // TILE):
            tile = dot(hid[own_rows, :], wall[:, i * TILE : (i + 1) * TILE]).astype(BF16)
            for k in range(TILE // 256):
                kv_out[i * (TILE // 256) + k] = tile[:, k * 256 : (k + 1) * 256]
        for d in range(1, G):
            j = member(d)
            copy = remote(
                kv_out.at[j],
                kv.at[slot(1 + me)],
                kv_send.at[d - 1],
                kv_recv.at[d - 1],
                {"sp": g * G + j},
            )
            send(copy)
            kv_done.append(copy)
        ctx_cross()
        tile = dot(hid[own_rows, :], wall[:, 2 * cols : 3 * cols]).astype(BF16)
        for j in range(G):
            q_out[j] = tile[:, j * 128 : (j + 1) * 128]
        for d in range(1, G):
            j = member(d)
            copy = remote(
                q_out.at[j],
                queries.at[me],
                q_send.at[d - 1],
                q_recv.at[d - 1],
                {"sp": g * G + j},
            )
            send(copy)
            q_done.append(copy)

    def ctx_slot(f, j):
        b = other(f) * G + j
        return pl.ds(pl.multiple_of(b * n_ctx, n_ctx), n_ctx)

    def ctx_project(f):
        hidden(ctx.at[f], hid_ctx, n_ctx, 1)
        for i in range(2 * cols // TILE):
            tile = dot(hid_ctx[...], wall[:, i * TILE : (i + 1) * TILE]).astype(BF16)
            for k in range(TILE // 256):
                c_out[f, i * (TILE // 256) + k] = tile[:, k * 256 : (k + 1) * 256]
        for d in range(1, G):
            j = member(d)
            n = f * (G - 1) + d - 1
            send(
                remote(
                    c_out.at[f, j],
                    ckv.at[ctx_slot(f, me)],
                    c_send.at[n],
                    c_recv.at[n],
                    {"sp": g * G + j},
                )
            )

    ctx_project(0)
    ctx_pass()
    if halved:
        tile = pair_dot(pl.ds(0, 2 * tokens), me, 0, 256)
        kv[half_slot(1 + member(1), 0), :] = tile[0:part_rows]
        kv[slot(1 + me), :] = tile[part_rows : part_rows + tokens]
        kv[half_slot(1 + member(2), 1), :] = tile[part_rows + tokens :]
        tile = pair_dot(pl.ds(0, 2 * tokens), me, 2 * cols, 128)
        queries[member(1), 0:part_rows, :] = tile[0:part_rows]
        queries[me] = tile[part_rows : part_rows + tokens]
        queries[member(2), part_rows:tokens, :] = tile[part_rows + tokens :]
    else:
        kv[slot(1 + me), :] = kv_out[me]
        queries[me] = q_out[me]
    ckv[ctx_slot(0, me), :] = c_out[0, me]
    gate[...] = dot(hid[own_rows, :], wall[:, 3 * cols : 4 * cols]).astype(BF16)
    for f in range(1, far):
        ctx_arrive(f)
        ctx_project(f)
        ckv[ctx_slot(f, me), :] = c_out[f, me]

    for copy in kv_done:
        copy.wait_recv()
    low = (WIN_ROWS // 2 - 1) * GRID_W
    send(
        remote(
            kv.at[slot(G)],
            kv.at[slot(0)],
            h_send.at[0],
            h_recv.at[0],
            {"sp": lax.rem(s + G, S)},
        ),
        g < far - 1,
    )
    send(
        remote(
            kv.at[pl.ds(tokens, low)],
            kv.at[pl.ds((G + 1) * tokens, low)],
            h_send.at[1],
            h_recv.at[1],
            {"sp": lax.rem(s + S - G, S)},
        ),
        g > 0,
    )

    @pl.when(g > 0)
    def _():
        ref = kv.at[slot(0)]
        remote(ref, ref, h_send.at[0], h_recv.at[0], partner).wait_recv()

    @pl.when(g < far - 1)
    def _():
        ref = kv.at[pl.ds((G + 1) * tokens, low)]
        remote(ref, ref, h_send.at[1], h_recv.at[1], partner).wait_recv()

    for f in range(far):
        for d in range(1, G):
            n = f * (G - 1) + d - 1
            ref = ckv.at[ctx_slot(f, member_back(d))]
            remote(ref, ref, c_send.at[n], c_recv.at[n], partner).wait_recv()
    for copy in q_done:
        copy.wait_recv()

    total_rows = rows * S
    band_rows = rows // X
    span = band_rows * GRID_W
    half = lax.broadcasted_iota(jnp.int32, (span, 128), 1) < 64
    scale = 0.125

    def token_rows(x):
        return pl.ds(pl.multiple_of(x * span, span), span)

    def attend(phase, x, first, last):
        @pl.loop(first, last)
        def _(d):
            b = lax.rem(me + 1 + d, G)
            q2 = queries[b, token_rows(x), :].astype(F32) * scale
            outs = []
            for e in range(2):
                q = jnp.where(half if e == 0 else jnp.logical_not(half), q2, 0.0).astype(BF16)
                sc = dot_t(q, ckv[:, 0:128])
                sw = []
                bands = []
                for r in range(band_rows):
                    row = (g * G + b) * rows + x * band_rows + r
                    rs = jnp.clip(row - WIN_ROWS // 2, 0, total_rows - WIN_ROWS)
                    band = pl.ds(
                        pl.multiple_of((rs - g * G * rows + rows) * GRID_W, GRID_W),
                        WIN_ROWS * GRID_W,
                    )
                    bands.append(band)
                    offsets = jnp.concatenate(
                        [
                            table[e, rs - row + WIN_ROWS - 1 + 2 * p]
                            for p in range(WIN_ROWS // 2)
                        ],
                        axis=1,
                    )
                    sw.append(dot_t(q[r * GRID_W : (r + 1) * GRID_W], kv[band, 0:128]) + offsets)
                sw = jnp.concatenate(sw, axis=0)
                m = jnp.maximum(
                    jnp.max(sc, axis=-1, keepdims=True), jnp.max(sw, axis=-1, keepdims=True)
                )
                pc = jnp.exp(sc - m)
                pw = jnp.exp(sw - m)
                total = jnp.sum(pc, axis=-1, keepdims=True) + jnp.sum(pw, axis=-1, keepdims=True)
                pw = pw.astype(BF16)
                o = dot(pc.astype(BF16), ckv[:, 128:256])
                ow = [
                    dot(pw[r * GRID_W : (r + 1) * GRID_W], kv[bands[r], 128:256])
                    for r in range(band_rows)
                ]
                outs.append((o + jnp.concatenate(ow, axis=0)) / total)
            att_out[b, token_rows(x), :] = jnp.where(half, outs[0], outs[1]).astype(BF16)

            @pl.when(d < G - 1)
            def _():
                give_back(phase, x, d).start()

    def give_back(phase, x, d):
        b = lax.rem(me + 1 + d, G)
        n = phase * G + d
        return remote(
            att_out.at[b, token_rows(x)],
            att.at[me, token_rows(x)],
            o_send.at[n],
            o_recv.at[n],
            {"sp": g * G + b},
        )

    own = tokens // T
    piece = width // GROUPS

    def project_out(phase, x):
        att[me, token_rows(x), :] = att_out[me, token_rows(x), :]
        for d in range(G - 1):
            give_back(phase, x, d).wait()
        for j in range(G):
            at = slice(j * 128, (j + 1) * 128)
            a = gate[token_rows(x), at].astype(F32)
            a = a / (1.0 + jnp.exp(-a)) * att[j, token_rows(x), :].astype(F32)
            gate[token_rows(x), at] = a.astype(BF16)
        copies = []
        for n in range(GROUPS):
            at = pl.ds(n * piece, piece)
            prod[phase, :, at] = dot(gate[token_rows(x), :], wo[:, at]).astype(BF16)
            copy = remote(
                prod.at[phase, pl.ds(pl.multiple_of((1 - core) * own, own), own), at],
                mate.at[phase, :, at],
                m_send.at[phase * GROUPS + n],
                m_recv.at[phase * GROUPS + n],
                partner,
            )
            copy.start()
            copies.append(copy)
        return copies

    mine = pl.ds(pl.multiple_of(core * own, own), own)

    def cross_send(phase, x, copies):
        crossing = []
        for n in range(GROUPS):
            at = pl.ds(n * piece, piece)
            copies[n].wait()
            both = prod[phase, mine, at].astype(F32) + mate[phase, :, at].astype(F32)
            cross[phase, :, at] = both.astype(BF16)
            copy = remote(
                cross.at[phase, :, at],
                terms.at[phase, :, at],
                r_send.at[phase * GROUPS + n],
                r_recv.at[phase * GROUPS + n],
                {"tp": x * 2 + core},
            )
            copy.start()
            crossing.append(copy)
        return crossing

    crossing = []
    order = [lax.rem(xi + phase + 1, X) for phase in range(X)]
    attend(0, order[0], 0, G)
    for phase in range(1, X):
        x, ahead = order[phase], order[phase - 1]
        attend(phase, x, 0, 1)
        copies = project_out(phase - 1, ahead)
        attend(phase, x, 1, G - 1)
        crossing.append(cross_send(phase - 1, ahead, copies))
        attend(phase, x, G - 1, G)
    copies = project_out(X - 1, order[X - 1])
    for n in range(GROUPS):
        at = pl.ds(n * piece, piece)
        copies[n].wait()
        total = prod[X - 1, mine, at].astype(F32) + mate[X - 1, :, at].astype(F32)
        for phase in range(X - 1):
            crossing[phase][n].wait()
            total = total + terms[phase, :, at].astype(F32)
        own_sum[:, at] = total.astype(BF16).astype(F32)
    b = own_sum[...]
    inv = lax.rsqrt(jnp.mean(b * b, axis=-1, keepdims=True) + EPSILON)
    own_at = pl.ds(pl.multiple_of(own_first + t * own, own), own)
    out[...] = (
        lat[own_at, :].astype(F32) + modrow[4:5, :] * (b * inv * gain_post[...])
    ).astype(BF16)

    for cond, copy in pending:
        if cond is None:
            copy.wait_send()
        else:

            @pl.when(cond)
            def _(copy=copy):
                copy.wait_send()


def layout_of(S, T):
    X = T // 2
    Y = X if S % X == 0 else 1
    return X, Y, S // Y


def grid_halved(S, T, G):
    return G == 4 and layout_of(S, T)[1] == 2


def shards(
    S,
    T,
    latent,
    context,
    condition,
    context_condition,
    gain_pre,
    gain_post,
    w_shift,
    w_scale,
    w_gate,
    w_query,
    w_key,
    w_value,
    w_silu,
    offset_bias,
    w_out,
):
    in_rows, cols = w_shift.shape
    tokens, width = latent.shape
    n_ctx = context.shape[0]
    heads = offset_bias.shape[0]
    turned = jnp.transpose(offset_bias, (1, 0, 2))
    pairs = turned.shape[0] - 1
    own_rows = tokens // T
    vmem = pl.BlockSpec(memory_space=pltpu.VMEM)
    hbm = pl.BlockSpec(memory_space=pl.ANY)
    sem = pltpu.SemaphoreType.DMA
    X = T // 2
    G = heads // 2
    far = S // G
    held = 2 * tokens if grid_halved(S, T, G) else tokens
    _, Y, Z = layout_of(S, T)
    return pl.pallas_call(
        functools.partial(kernel, S, T),
        out_shape=jax.ShapeDtypeStruct((own_rows, width), BF16),
        in_specs=[hbm] * 15,
        out_specs=vmem,
        scratch_shapes=[
            pltpu.VMEM((width,), BF16),
            pltpu.VMEM((width,), BF16),
            pltpu.VMEM((16, width), F32),
            pltpu.VMEM((1, width), F32),
            pltpu.VMEM((1, width), F32),
            pltpu.VMEM(turned.shape, F32),
            pltpu.VMEM((pairs, heads, 2 * GRID_W), F32),
            pltpu.VMEM((held, width), BF16),
            pltpu.VMEM((far, n_ctx, width), BF16),
            pltpu.VMEM((3, in_rows, cols), BF16),
            pltpu.VMEM((width, 4 * cols), BF16),
            pltpu.VMEM((cols, width), BF16),
            pltpu.VMEM((8, cols), F32),
            pltpu.VMEM((S, 8, cols), F32),
            pltpu.VMEM((T, 8, cols), F32),
            pltpu.VMEM((8, width), F32),
            pltpu.VMEM((held + n_ctx, width), BF16),
            pltpu.VMEM((G, tokens, 256), BF16),
            pltpu.VMEM((G, tokens, 128), BF16),
            pltpu.VMEM((far, G, n_ctx, 256), BF16),
            pltpu.VMEM(((G + 2) * tokens, 256), BF16),
            pltpu.VMEM((G, tokens, 128), BF16),
            pltpu.VMEM((S * n_ctx, 256), BF16),
            pltpu.VMEM((tokens, cols), BF16),
            pltpu.VMEM((2, pairs, GRID_W, 2 * GRID_W), F32),
            pltpu.VMEM((G, tokens, 128), BF16),
            pltpu.VMEM((G, tokens, 128), BF16),
            pltpu.VMEM((X, tokens // X, width), BF16),
            pltpu.VMEM((X, own_rows, width), BF16),
            pltpu.VMEM((own_rows, width), F32),
            pltpu.VMEM((max(X - 1, 1), own_rows, width), BF16),
            pltpu.VMEM((max(X - 1, 1), own_rows, width), BF16),
            sem((13 + 2 * G,)),
            pltpu.SemaphoreType.REGULAR((max(Y + Z - 3, 1),)),
            sem((max(S - 1, 1),)),
            sem((max(S - 1, 1),)),
            sem((max(T - 1, 1),)),
            sem((max(T - 1, 1),)),
            sem((max(far - 1, 1),)),
            sem((max(far - 1, 1),)),
            sem((max((far - 1) * (X - 1), 1),)),
            sem((max((far - 1) * (X - 1), 1),)),
            sem((max((far - 1) * X, 1),)),
            sem((max((far - 1) * X, 1),)),
            sem((2 * PIECES,)),
            sem((2 * PIECES,)),
            sem((2,)),
            sem((2,)),
            sem((G,)),
            sem((G,)),
            sem((G,)),
            sem((G,)),
            sem((max(far * (G - 1), 1),)),
            sem((max(far * (G - 1), 1),)),
            sem((2,)),
            sem((2,)),
            sem((X * G,)),
            sem((X * G,)),
            sem((X * GROUPS,)),
            sem((X * GROUPS,)),
            sem((max(X - 1, 1) * GROUPS,)),
            sem((max(X - 1, 1) * GROUPS,)),
        ],
        compiler_params=pltpu.CompilerParams(
            collective_id=0, has_side_effects=True, vmem_limit_bytes=60 * 1024 * 1024
        ),
    )(
        condition,
        context_condition,
        gain_pre.reshape(1, width),
        gain_post.reshape(1, width),
        turned,
        latent,
        context,
        w_shift,
        w_scale,
        w_gate,
        w_query,
        w_key,
        w_value,
        w_silu,
        w_out,
    )


def solution(mesh):
    in_specs = (
        P("sp", None),
        P("sp", None),
        P(),
        P(),
        P(),
        P(),
        P("sp", "tp"),
        P("sp", "tp"),
        P("sp", "tp"),
        P(None, "tp"),
        P(None, "tp"),
        P(None, "tp"),
        P(None, "tp"),
        P("tp", None, None),
        P("tp", None),
    )
    return jax.shard_map(
        functools.partial(shards, mesh.shape["sp"], mesh.shape["tp"]),
        mesh=mesh,
        in_specs=in_specs,
        out_specs=P(("sp", "tp"), None),
        check_vma=False,
    )
```
